32 devices in a mesh: ep: 8 (over z, x), tp: 4 (over y, core).
Axes of the slice: x: 2, y: 2, z: 4, core: 2. Of those that a mesh axis runs over, the one named last changes fastest.
Arguments:
- tokens: bfloat16 [64, 2048], P('ep'), may hold values from -6 to 6
- mix_gain: bfloat16 [2048], replicated, may hold values from 0.099609375 to 1.8984375
- w_query: bfloat16 [2048, 512], P(None, 'tp'), may hold values from -0.125 to 0.125
- w_key: bfloat16 [2048, 512], P(None, 'tp'), may hold values from -0.125 to 0.125
- w_value: bfloat16 [2048, 512], P(None, 'tp'), may hold values from -0.125 to 0.125
- w_igate: bfloat16 [2048, 4], replicated, may hold values from -0.125 to 0.125
- w_fgate: bfloat16 [2048, 4], replicated, may hold values from -0.125 to 0.125
- forget_bias: float32 [4], replicated, may hold values from 0.5 to 4.5
- w_out: bfloat16 [512, 2048], P('tp'), may hold values from -0.25 to 0.25
- mem_state: float32 [64, 4, 16384], P('ep', 'tp'), may hold values from -0.75 to 0.75
- norm_state: float32 [64, 512], P('ep', 'tp'), may hold values from -0.75 to 0.75
- max_state: float32 [64, 4], P('ep', 'tp'), may hold values from -3 to 3
- ffn_gain: bfloat16 [2048], replicated, may hold values from 0.099609375 to 1.8984375
- route_ids: int32 [64, 2], P('ep'), may hold values from 0 to 7, all different within a row; in each aligned block of 8 rows (0 to 7, 8 to 15, ...) at most 3 rows name the same one
- route_weights: float32 [64, 2], P('ep'), may hold values from 0.1 to 1
- w_gate: bfloat16 [2048, 32768], P(None, ('ep', 'tp')), may hold values from -0.125 to 0.125
- w_up: bfloat16 [2048, 32768], P(None, ('ep', 'tp')), may hold values from -0.125 to 0.125
- w_down: bfloat16 [32768, 2048], P('ep', 'tp'), may hold values from -0.09375 to 0.09375
Outputs:
- out_tokens: bfloat16 [64, 2048], P('ep', 'tp')
- new_memory: float32 [64, 4, 16384], P('ep', 'tp')
- new_norm: float32 [64, 512], P('ep', 'tp')
- new_max: float32 [64, 4], P('ep', 'tp')
The draws below stay inside these ranges and needn't reach their ends.
Inputs may be any that keep to these rules, and one draw needn't show every extreme that they name: `route_ids`: each row names 2 different experts; among the rows of one index of ep no expert is named more than 3 times, a bound that some block reaches.
All inputs are finite; a program needn't handle non-finite values.
Results may differ from the reference program's by a relative error of at most 0.013.
The reference program's roundings to bfloat16 on the way (of `normed`, `query_rows`, `readout`, `residual`, `normed_ffn` and `hidden`) count: a program that leaves them out, or rounds other values in their place, can miss the bound.
Values may be sent and summed in bfloat16 or wider, within the bound.
No kernel may reach another device: no remote copies, remote signals or barrier semaphores. Data moves between devices by JAX's collectives and lax.ppermute only.
A program may use at most 64 MiB of HBM per device.

```python
import math
import jax
import jax.numpy as jnp
import numpy as np
from jax import lax

D = 2048
HEADS = 4
HEAD_DIM = 128
FF = 4096
TOPK = 2
SEQ_DEV = 8
EXPERTS = 8
CAP = 3
BATCH = 64
N_EP = 8
N_TP = 4


def steps_of(stream_key, shape, pieces, low, top_value):
    factor_of, own = 1.0, jax.random.fold_in(stream_key, 6)
    for dim, parts in pieces:
        heights = jnp.exp(jax.random.uniform(jax.random.fold_in(own, dim), (parts,), jnp.float32, low / len(pieces), top_value / len(pieces)))
        factor_of = factor_of * jnp.repeat(heights, shape[dim] // parts).reshape([-1 if axis == dim else 1 for axis in range(len(shape))])
    return factor_of


def assign_block(own_key, own, number, rows, number_of, top, limit, slope):
    ranking = jax.random.permutation(own_key, number_of)
    packed, ordinary = portions_of(number_of, rows * top, limit, slope, True), portions_of(number_of, rows * top, limit, slope, False)
    places = jnp.arange(number_of)

    def named(lengths, offset_by):
        used = int((lengths > 0).sum())
        fixed = max(1, used // 4)
        shifted = fixed + (places - fixed + offset_by * (used - fixed)) % max(1, number_of - fixed)
        return jnp.zeros((number_of,), jnp.int32).at[ranking[jnp.where(places < fixed, places, shifted)]].set(jnp.asarray(lengths, jnp.int32))

    lengths = jnp.where(number % 4 == 0, named(packed, number // 4), named(ordinary, number - number // 4 - 1))
    mixed = jax.random.permutation(jax.random.fold_in(own, 3), number_of)
    donor, sink = mixed[0:number_of // 2 * 2:2], mixed[1:number_of // 2 * 2:2]
    slack = jnp.minimum(lengths[donor] - 1, limit - lengths[sink]) // 2
    slack = jnp.where((donor == ranking[0]) | (sink == ranking[0]) | (lengths[sink] == 0), 0, jnp.maximum(slack, 0))
    shifted = jax.random.randint(jax.random.fold_in(own, 4), (number_of // 2,), 0, 1 << 20) % (slack + 1)
    lengths = lengths.at[donor].add(-shifted).at[sink].add(shifted)
    items = jnp.searchsorted(jnp.cumsum(lengths), jnp.arange(rows * top), side="right").astype(jnp.int32)
    grid = items.reshape(top, rows).T
    grid = grid[jax.random.permutation(jax.random.fold_in(own, 1), rows)]
    offset_by = jax.random.randint(jax.random.fold_in(own, 2), (rows, 1), 0, top)
    return jnp.take_along_axis(grid, (jnp.arange(top)[None, :] + offset_by) % top, axis=1)


def portions_of(number_of, total, most, lean, full):
    weights = [(1 << 20) // math.isqrt(rank ** lean) + 1 for rank in range(1, number_of + 1)]
    largest = most if full else min(most, max(-(-total // number_of), total * weights[0] // sum(weights)))
    least = 1 if total - largest >= number_of - 1 else 0
    given, surplus = [largest] + [least] * (number_of - 1), total - largest - least * (number_of - 1)
    while surplus > 0:
        free = [i for i in range(1, number_of) if given[i] < largest] or [i for i in range(1, number_of) if given[i] < most]
        whole, budget = sum([weights[i] for i in free]), surplus
        for i in free:
            more = min(most - given[i], max(1, budget * weights[i] // whole), surplus)
            given[i] = given[i] + more
            surplus = surplus - more
    return np.array(given)


def gaussian(stream_key, shape, scale, most, pieces=(), held_as=jnp.bfloat16):
    factor_of = steps_of(stream_key, shape, pieces, -0.22, 0.18) if pieces else 1.0
    result = jax.random.normal(stream_key, shape, jnp.float32) * scale * factor_of
    return jnp.minimum(jnp.maximum(result, -most), most).astype(held_as)


def setup_inputs(seed: int = 0) -> dict:
    keys = jax.random.split(jax.random.key(seed), 19)
    tokens = gaussian(keys[0], (BATCH, D), 1.0, 6.0, ((0, 8),))
    mix_gain = jnp.clip(1.0 + 0.18 * jax.random.normal(keys[1], (D,), jnp.float32), 0.099609375, 1.8984375).astype(jnp.bfloat16)
    w_query = gaussian(keys[2], (D, HEADS * HEAD_DIM), D ** -0.5, 0.125, ((1, 4),))
    w_key = gaussian(keys[3], (D, HEADS * HEAD_DIM), D ** -0.5, 0.125, ((1, 4),))
    w_value = gaussian(keys[4], (D, HEADS * HEAD_DIM), D ** -0.5, 0.125, ((1, 4),))
    w_igate = gaussian(keys[5], (D, HEADS), D ** -0.5, 0.125)
    w_fgate = gaussian(keys[6], (D, HEADS), D ** -0.5, 0.125)
    forget_bias = jnp.clip(jax.random.uniform(keys[7], (HEADS,), jnp.float32, 0.5, 4.5), 0.5, 4.5)
    w_out = gaussian(keys[8], (HEADS * HEAD_DIM, D), (HEADS * HEAD_DIM) ** -0.5, 0.25, ((0, 4),))
    mem_state = gaussian(keys[9], (BATCH, HEADS, HEAD_DIM * HEAD_DIM), 0.125, 0.75, ((0, 8), (1, 4)), jnp.float32)
    norm_state = gaussian(keys[10], (BATCH, HEADS * HEAD_DIM), 0.125, 0.75, ((0, 8), (1, 4)), jnp.float32)
    max_state = jnp.clip(jax.random.uniform(keys[11], (BATCH, HEADS), jnp.float32, -3.0, 3.0) * steps_of(keys[11], (BATCH, HEADS), ((0, 8), (1, 4)), -0.4, 0.0), -3.0, 3.0)
    ffn_gain = jnp.clip(1.0 + 0.18 * jax.random.normal(keys[12], (D,), jnp.float32), 0.099609375, 1.8984375).astype(jnp.bfloat16)
    route_ids_keys = jax.random.split(jax.random.fold_in(keys[13], 1), BATCH // SEQ_DEV)
    route_ids_turns = jax.random.permutation(jax.random.fold_in(keys[13], 3), BATCH // SEQ_DEV)
    route_ids = jax.vmap(lambda own, number: assign_block(jax.random.fold_in(keys[13], 2), own, number, SEQ_DEV, EXPERTS, TOPK, CAP, 2))(route_ids_keys, route_ids_turns).reshape((BATCH, TOPK))
    route_weights = jnp.clip(jnp.exp(math.log(1.0) - 2.3025851 * jax.random.uniform(keys[14], (BATCH, TOPK), jnp.float32) ** steps_of(keys[14], (BATCH, TOPK), ((0, 8),), -0.2, 0.2)), 0.1, 1.0)
    w_gate = gaussian(keys[15], (D, EXPERTS * FF), D ** -0.5, 0.125, ((1, 32),))
    w_up = gaussian(keys[16], (D, EXPERTS * FF), D ** -0.5, 0.125, ((1, 32),))
    w_down = gaussian(keys[17], (EXPERTS * FF, D), FF ** -0.5, 0.09375, ((0, 8), (1, 4)))
    return dict(tokens=tokens, mix_gain=mix_gain, w_query=w_query, w_key=w_key, w_value=w_value, w_igate=w_igate, w_fgate=w_fgate, forget_bias=forget_bias, w_out=w_out, mem_state=mem_state, norm_state=norm_state, max_state=max_state, ffn_gain=ffn_gain, route_ids=route_ids, route_weights=route_weights, w_gate=w_gate, w_up=w_up, w_down=w_down)


epsilon = 1e-06

def scaled_rows(row_data, gain_values):
    squares = lax.optimization_barrier(jnp.mean(row_data * row_data, axis=1, keepdims=True))
    return (row_data * lax.rsqrt(squares + epsilon) * gain_values.astype(jnp.float32)).astype(jnp.bfloat16)

def rounded_wide(matrix):
    return lax.optimization_barrier(matrix.astype(jnp.bfloat16)).astype(jnp.float32)

def reference(tokens, mix_gain, w_query, w_key, w_value, w_igate, w_fgate, forget_bias, w_out, mem_state, norm_state, max_state, ffn_gain, route_ids, route_weights, w_gate, w_up, w_down):
    residual_in = tokens.astype(jnp.float32)
    normed = scaled_rows(residual_in, mix_gain)
    query_rows = rounded_wide(jnp.dot(normed, w_query, preferred_element_type=jnp.float32)).reshape(BATCH, HEADS, HEAD_DIM)
    key_rows = rounded_wide(jnp.dot(normed, w_key, preferred_element_type=jnp.float32)).reshape(BATCH, HEADS, HEAD_DIM)
    key_rows = key_rows * HEAD_DIM ** (-0.5)
    value_rows = rounded_wide(jnp.dot(normed, w_value, preferred_element_type=jnp.float32)).reshape(BATCH, HEADS, HEAD_DIM)
    input_gate = jnp.dot(normed, w_igate, preferred_element_type=jnp.float32)
    forget_log = jax.nn.log_sigmoid(jnp.dot(normed, w_fgate, preferred_element_type=jnp.float32) + forget_bias[None, :])
    new_max = jnp.maximum(forget_log + max_state, input_gate)
    keep_weight = jnp.exp(forget_log + max_state - new_max)
    new_weight = jnp.exp(input_gate - new_max)
    memory = mem_state.reshape(BATCH, HEADS, HEAD_DIM, HEAD_DIM)
    new_memory = keep_weight[:, :, None, None] * memory + new_weight[:, :, None, None] * key_rows[:, :, :, None] * value_rows[:, :, None, :]
    new_norm = keep_weight[:, :, None] * norm_state.reshape(BATCH, HEADS, HEAD_DIM) + new_weight[:, :, None] * key_rows
    numerator = jnp.einsum('bhd,bhde->bhe', query_rows, new_memory, precision=lax.Precision.HIGHEST)
    denominator = lax.optimization_barrier(jnp.sum(query_rows * new_norm, axis=2))
    readout = (numerator / jnp.maximum(jnp.abs(denominator), jnp.exp(-new_max))[:, :, None]).astype(jnp.bfloat16)
    readout = readout.reshape(BATCH, HEADS * HEAD_DIM)
    group_width = HEADS * HEAD_DIM // N_TP
    head_total = jnp.zeros((BATCH, D), jnp.float32)
    for group_at in range(N_TP):
        group_start = group_at * group_width
        product = jnp.dot(readout[:, group_start:group_start + group_width], w_out[group_start:group_start + group_width], preferred_element_type=jnp.float32)
        head_total = head_total + rounded_wide(product)
    residual = (residual_in + head_total).astype(jnp.bfloat16)
    residual_wide = lax.optimization_barrier(residual).astype(jnp.float32)
    normed_ffn = scaled_rows(residual_wide, ffn_gain)
    route_bound = N_EP * CAP
    flat_ids = route_ids.reshape(-1)
    flat_weights = route_weights.reshape(-1)

    def one_expert(running, expert_at):
        matches = flat_ids == expert_at
        places = jnp.nonzero(matches, size=route_bound, fill_value=0)[0].astype(jnp.int32)
        live = (jnp.arange(route_bound, dtype=jnp.int32) < jnp.sum(matches.astype(jnp.int32))).astype(jnp.float32)
        token_at = places // TOPK
        picked = jnp.take(normed_ffn, token_at, axis=0)
        start = (expert_at * FF).astype(jnp.int32)
        gate_sum = jnp.dot(picked, lax.dynamic_slice_in_dim(w_gate, start, FF, 1), preferred_element_type=jnp.float32)
        up_sum = jnp.dot(picked, lax.dynamic_slice_in_dim(w_up, start, FF, 1), preferred_element_type=jnp.float32)
        hidden = (jax.nn.silu(gate_sum) * up_sum).astype(jnp.bfloat16)
        expert_out = jnp.dot(hidden, lax.dynamic_slice_in_dim(w_down, start, FF, 0), preferred_element_type=jnp.float32)
        scale = jnp.take(flat_weights, places) * live
        return (running.at[token_at].add(expert_out * scale[:, None]), None)
    routed, unused = lax.scan(one_expert, jnp.zeros((BATCH, D), jnp.float32), jnp.arange(EXPERTS, dtype=jnp.int32))
    out_tokens = (residual_wide + routed).astype(jnp.bfloat16)
    return (out_tokens, new_memory.reshape(BATCH, HEADS, HEAD_DIM * HEAD_DIM), new_norm.reshape(BATCH, HEADS * HEAD_DIM), new_max)
```

```python
import functools
import jax
import jax.numpy as jnp
from jax import lax
from jax.experimental import pallas as pl
from jax.experimental.pallas import tpu as pltpu
from jax.sharding import PartitionSpec as P

FF = 4096
LANES = 128
epsilon = 1e-06
f32 = jnp.float32
bf16 = jnp.bfloat16


VMEM = pl.BlockSpec(memory_space=pltpu.VMEM)
ANY = pl.BlockSpec(memory_space=pl.ANY)


def kernel_call(body, outs, ins, in_specs=None, out_specs=None, scratch=(), cost=1000, limit=None):
    return pl.pallas_call(
        body,
        out_shape=outs,
        in_specs=in_specs or [VMEM] * len(ins),
        out_specs=out_specs or tuple([VMEM] * len(outs)),
        scratch_shapes=list(scratch),
        compiler_params=pltpu.CompilerParams(vmem_limit_bytes=limit),
        cost_estimate=pl.CostEstimate(flops=cost, bytes_accessed=0, transcendentals=0),
    )(*ins)


def scaled_tiles(wide, gain_ref):
    width = wide.shape[1]
    factor = lax.rsqrt(jnp.sum(wide * wide, 1, keepdims=True) / width + epsilon)
    gain = gain_ref[...].astype(f32)
    tiles = [
        wide[:, at * LANES : (at + 1) * LANES] * factor * gain[at : at + 1, :]
        for at in range(width // LANES)
    ]
    return jnp.concatenate(tiles, 1).astype(bf16)


def to_column(row):
    count = row.shape[1]
    eye = lax.broadcasted_iota(jnp.int32, (count, count), 0) == lax.broadcasted_iota(
        jnp.int32, (count, count), 1
    )
    return jnp.sum(jnp.where(eye, jnp.broadcast_to(row, (count, count)), 0.0), 1, keepdims=True)


def to_row(column):
    count = column.shape[0]
    eye = lax.broadcasted_iota(jnp.int32, (count, count), 0) == lax.broadcasted_iota(
        jnp.int32, (count, count), 1
    )
    return jnp.sum(jnp.where(eye, jnp.broadcast_to(column, (count, count)), 0.0), 0, keepdims=True)


def routing(ids, weights, rows, slots, spans):
    top_count, seq_count = ids.shape
    at = lax.broadcasted_iota(jnp.int32, (rows, seq_count), 0)
    expert = at // (slots * spans)
    slot = (at % slots).astype(f32)
    named = jnp.zeros((rows, seq_count), f32)
    weighted = jnp.zeros((rows, seq_count), f32)
    for k in range(top_count):
        hit = expert == ids[k : k + 1, :]
        named = named + jnp.where(hit, 1.0, 0.0)
        weighted = weighted + jnp.where(hit, weights[k : k + 1, :], 0.0)
    before = jnp.where(
        lax.broadcasted_iota(jnp.int32, (seq_count, seq_count), 0)
        < lax.broadcasted_iota(jnp.int32, (seq_count, seq_count), 1),
        1.0,
        0.0,
    )
    rank = jnp.dot(named, before, preferred_element_type=f32)
    mine = rank == slot
    return jnp.where(mine, named, 0.0), jnp.where(mine, weighted, 0.0)


def cell_kernel(
    slots, spans,
    tokens_ref, gain_ref, wq_ref, wk_ref, wv_ref, wi_ref, wf_ref, bias_ref, mem_ref, norm_ref, max_ref, wo_ref,
    ids_ref, weights_ref,
    partial_ref, keys_ref, values_ref, keep_ref, fresh_ref, norm_out, max_out, placing_ref, mixing_ref,
):
    head = lax.axis_index("tp")
    seq_count = tokens_ref.shape[0]
    head_dim = wq_ref.shape[1]
    normed = scaled_tiles(tokens_ref[...].astype(f32), gain_ref)

    def project(ref):
        return jnp.dot(normed, ref[...], preferred_element_type=f32).astype(bf16).astype(f32)

    def gate(ref):
        return lax.dot_general(
            normed, ref[...], (((1,), (1,)), ((), ())), preferred_element_type=f32
        )

    query, key, value = project(wq_ref), project(wk_ref) * head_dim ** (-0.5), project(wv_ref)
    inputs = gate(wi_ref)
    forgets = gate(wf_ref) + bias_ref[...]
    here = lax.broadcasted_iota(jnp.int32, inputs.shape, 1) == head
    input_gate = jnp.sum(jnp.where(here, inputs, 0.0), 1, keepdims=True)
    forget = jnp.sum(jnp.where(here, forgets, 0.0), 1, keepdims=True)
    forget_log = jnp.minimum(forget, 0.0) - jnp.log1p(jnp.exp(-jnp.abs(forget)))
    held = forget_log + to_column(max_ref[...])
    new_max = jnp.maximum(held, input_gate)
    keep = jnp.exp(held - new_max)
    fresh = jnp.exp(input_gate - new_max)
    new_norm = keep * norm_ref[...] + fresh * key
    norm_out[...] = new_norm
    max_out[...] = to_row(new_max)
    keys_ref[...] = fresh * key
    values_ref[...] = value
    keep_ref[...] = jnp.broadcast_to(keep, keep_ref.shape)
    fresh_ref[...] = jnp.broadcast_to(fresh, fresh_ref.shape)
    query_t = query.T
    read = []
    for s in range(seq_count):
        read.append(jnp.sum(mem_ref[s] * query_t[:, s : s + 1], 0, keepdims=True))
    read = jnp.concatenate(read, 0)
    match = jnp.sum(query * key, 1, keepdims=True)
    numerator = keep * read + (fresh * match) * value
    denominator = jnp.sum(query * new_norm, 1, keepdims=True)
    readout = numerator / jnp.maximum(jnp.abs(denominator), jnp.exp(-new_max))
    partial_ref[...] = jnp.dot(
        readout.astype(bf16), wo_ref[...], preferred_element_type=f32
    ).astype(bf16)
    placing, mixing = routing(ids_ref[...], weights_ref[...], placing_ref.shape[0], slots, spans)
    placing_ref[...] = placing.astype(bf16)
    mixing_ref[...] = mixing


def pack_kernel(tokens_ref, gain_ref, placing_ref, *refs):
    *partials, packed_ref, residual_ref, tick_ref = refs
    total = partials[0][...].astype(f32)
    for ref in partials[1:]:
        total = total + ref[...].astype(f32)
    residual = (tokens_ref[...].astype(f32) + total).astype(bf16)
    residual_ref[...] = residual
    normed = scaled_tiles(residual.astype(f32), gain_ref)
    rows = jnp.dot(placing_ref[...], normed, preferred_element_type=f32)
    slots = packed_ref.shape[1]
    for at in range(packed_ref.shape[0]):
        packed_ref[at] = rows[at * slots : (at + 1) * slots, :].astype(bf16)
    tick_ref[...] = jnp.zeros(tick_ref.shape, f32)


def fetch_kernel(*refs):
    count = (len(refs) - 2) // 2
    sources, targets, sems = refs[1 : 1 + count], refs[1 + count : 1 + 2 * count], refs[-1]
    copies = [pltpu.make_async_copy(a, b, sems.at[i]) for i, (a, b) in enumerate(zip(sources, targets))]
    for copy in copies:
        copy.start()
    for copy in copies:
        copy.wait()


def down_kernel(tp_count, *refs):
    hiddens, weight_ref, out_ref, tick_ref = refs[:tp_count], refs[tp_count], refs[-2], refs[-1]
    me = lax.axis_index("tp")
    units = hiddens[0].shape[1]
    total = None
    for k in range(tp_count):
        start = pl.multiple_of(lax.rem(me + k, tp_count) * units, units)
        term = jnp.dot(
            hiddens[k][...], weight_ref[pl.ds(start, units), :], preferred_element_type=f32
        )
        total = term if total is None else total + term
    slots = out_ref.shape[1]
    for at in range(out_ref.shape[0]):
        out_ref[at] = total[at * slots : (at + 1) * slots, :].astype(bf16)
    tick_ref[...] = jnp.zeros(tick_ref.shape, f32)


def state_kernel(tick_ref, mem_ref, keys_ref, values_ref, keep_ref, out_ref):
    keys_t = keys_ref[...].T
    value = values_ref[...]
    for s in range(mem_ref.shape[0]):
        out_ref[s] = (
            keep_ref[s : s + 1, :] * mem_ref[s] + keys_t[:, s : s + 1] * value[s : s + 1, :]
        )


def final_kernel(residual_ref, mixing_ref, returned_ref, out_ref):
    width = out_ref.shape[1]
    start = pl.multiple_of(lax.axis_index("tp") * width, width)
    routed = lax.dot_general(
        mixing_ref[...],
        returned_ref[...].astype(f32),
        (((0,), (0,)), ((), ())),
        precision=lax.Precision.HIGHEST,
        preferred_element_type=f32,
    )
    out_ref[...] = (residual_ref[:, pl.ds(start, width)].astype(f32) + routed).astype(bf16)


def from_ahead(value, count):
    return [value] + [
        lax.ppermute(value, "tp", [((at + k) % count, at) for at in range(count)])
        for k in range(1, count)
    ]


def shards(
    tokens, mix_gain, w_query, w_key, w_value, w_igate, w_fgate, forget_bias, w_out, mem_state, norm_state,
    max_state, ffn_gain, route_ids, route_weights, w_gate, w_up, w_down,
):
    seq_count, model_width = tokens.shape
    head_dim = norm_state.shape[1]
    tp_count = lax.axis_size("tp")
    ep_count = lax.axis_size("ep")
    own_width = model_width // tp_count
    top_count = route_ids.shape[1]
    spans = FF // w_down.shape[0]
    experts = ep_count // spans
    bound = max(2, 3 * seq_count * top_count // (2 * experts))
    slots = bound + bound % 2
    rows = ep_count * slots
    struct = jax.ShapeDtypeStruct

    memory = mem_state.reshape(seq_count, head_dim, head_dim)
    gain_a = mix_gain.reshape(model_width // LANES, LANES)
    gain_b = ffn_gain.reshape(model_width // LANES, LANES)
    partial, keys, values, keep, fresh, new_norm, new_max, placing, mixing = kernel_call(
        functools.partial(cell_kernel, slots, spans),
        (
            pltpu.VMEM((seq_count, model_width), bf16),
            pltpu.VMEM((seq_count, head_dim), f32),
            pltpu.VMEM((seq_count, head_dim), f32),
            pltpu.VMEM((seq_count, head_dim), f32),
            pltpu.VMEM((seq_count, head_dim), f32),
            struct((seq_count, head_dim), f32),
            struct((1, seq_count), f32),
            pltpu.VMEM((rows, seq_count), bf16),
            pltpu.VMEM((rows, seq_count), f32),
        ),
        (
            tokens, gain_a, w_query, w_key, w_value, w_igate.T, w_fgate.T, forget_bias.reshape(1, -1), memory,
            norm_state, max_state.T, w_out, route_ids.T, route_weights.T,
        ),
        limit=16 << 20,
    )
    partials = from_ahead(partial, tp_count)
    packed, residual, tick = kernel_call(
        pack_kernel,
        (
            pltpu.VMEM((ep_count, slots, model_width), bf16),
            pltpu.VMEM((seq_count, model_width), bf16),
            pltpu.VMEM((8, LANES), f32),
        ),
        (tokens, gain_b, placing, *partials),
        limit=16 << 20,
    )
    arrived = lax.all_to_all(packed, "ep", split_axis=0, concat_axis=0, tiled=True)
    gate_w, up_w, down_w = kernel_call(
        fetch_kernel,
        tuple(pltpu.VMEM(w.shape, w.dtype) for w in (w_gate, w_up, w_down)),
        (tick, w_gate, w_up, w_down),
        in_specs=[ANY, *[pl.BlockSpec(memory_space=pltpu.HBM)] * 3],
        out_specs=(ANY,) * 3,
        scratch=[pltpu.SemaphoreType.DMA((3,))],
        cost=20_000_000,
        limit=1 << 20,
    )
    flat = arrived.reshape(rows, model_width)
    gate_sum = jnp.dot(flat, gate_w, preferred_element_type=f32)
    up_sum = jnp.dot(flat, up_w, preferred_element_type=f32)
    hidden = (jax.nn.silu(gate_sum) * up_sum).astype(bf16)
    hiddens = from_ahead(hidden, tp_count)
    outgoing, tock = kernel_call(
        functools.partial(down_kernel, tp_count),
        (pltpu.VMEM((ep_count, slots, own_width), bf16), pltpu.VMEM((8, LANES), f32)),
        (*hiddens, down_w),
        limit=16 << 20,
    )
    returned = lax.all_to_all(outgoing, "ep", split_axis=0, concat_axis=0, tiled=True)
    (new_memory,) = kernel_call(
        state_kernel,
        (struct((seq_count, head_dim, head_dim), f32),),
        (tock, memory, keys, values, keep),
        cost=20_000_000,
        limit=16 << 20,
    )
    (out_tokens,) = kernel_call(
        final_kernel,
        (struct((seq_count, own_width), bf16),),
        (residual, mixing, returned.reshape(rows, own_width)),
        limit=16 << 20,
    )
    return (
        out_tokens,
        new_memory.reshape(mem_state.shape),
        new_norm,
        new_max.T,
    )


def solution(mesh):
    placed = (
        P("ep", None),
        P(),
        P(None, "tp"),
        P(None, "tp"),
        P(None, "tp"),
        P(),
        P(),
        P(),
        P("tp", None),
        P("ep", "tp", None),
        P("ep", "tp"),
        P("ep", "tp"),
        P(),
        P("ep", None),
        P("ep", None),
        P(None, ("ep", "tp")),
        P(None, ("ep", "tp")),
        P("ep", "tp"),
    )
    return jax.shard_map(
        shards,
        mesh=mesh,
        in_specs=placed,
        out_specs=(P("ep", "tp"), P("ep", "tp", None), P("ep", "tp"), P("ep", "tp")),
        check_vma=False,
    )
```

```python
import functools
import jax
import jax.numpy as jnp
from jax import lax
from jax.experimental import pallas as pl
from jax.experimental.pallas import tpu as pltpu
from jax.sharding import PartitionSpec as P

FF = 4096
LANES = 128
epsilon = 1e-06
f32 = jnp.float32
bf16 = jnp.bfloat16


VMEM = pl.BlockSpec(memory_space=pltpu.VMEM)
ANY = pl.BlockSpec(memory_space=pl.ANY)


def kernel_call(body, outs, ins, in_specs=None, out_specs=None, scratch=(), cost=1000, limit=None):
    return pl.pallas_call(
        body,
        out_shape=outs,
        in_specs=in_specs or [VMEM] * len(ins),
        out_specs=out_specs or tuple([VMEM] * len(outs)),
        scratch_shapes=list(scratch),
        compiler_params=pltpu.CompilerParams(vmem_limit_bytes=limit),
        cost_estimate=pl.CostEstimate(flops=cost, bytes_accessed=0, transcendentals=0),
    )(*ins)


def scaled_tiles(wide, gain_ref):
    width = wide.shape[1]
    factor = lax.rsqrt(jnp.sum(wide * wide, 1, keepdims=True) / width + epsilon)
    gain = gain_ref[...].astype(f32)
    tiles = [
        wide[:, at * LANES : (at + 1) * LANES] * factor * gain[at : at + 1, :]
        for at in range(width // LANES)
    ]
    return jnp.concatenate(tiles, 1).astype(bf16)


def to_column(row):
    count = row.shape[1]
    eye = lax.broadcasted_iota(jnp.int32, (count, count), 0) == lax.broadcasted_iota(
        jnp.int32, (count, count), 1
    )
    return jnp.sum(jnp.where(eye, jnp.broadcast_to(row, (count, count)), 0.0), 1, keepdims=True)


def to_row(column):
    count = column.shape[0]
    eye = lax.broadcasted_iota(jnp.int32, (count, count), 0) == lax.broadcasted_iota(
        jnp.int32, (count, count), 1
    )
    return jnp.sum(jnp.where(eye, jnp.broadcast_to(column, (count, count)), 0.0), 0, keepdims=True)


def routing(ids, weights, rows, slots, spans, base):
    top_count, seq_count = ids.shape
    at = lax.broadcasted_iota(jnp.int32, (rows, seq_count), 0)
    expert = ((at // slots) ^ base) // spans
    slot = (at % slots).astype(f32)
    named = jnp.zeros((rows, seq_count), f32)
    weighted = jnp.zeros((rows, seq_count), f32)
    for k in range(top_count):
        hit = expert == ids[k : k + 1, :]
        named = named + jnp.where(hit, 1.0, 0.0)
        weighted = weighted + jnp.where(hit, weights[k : k + 1, :], 0.0)
    before = jnp.where(
        lax.broadcasted_iota(jnp.int32, (seq_count, seq_count), 0)
        < lax.broadcasted_iota(jnp.int32, (seq_count, seq_count), 1),
        1.0,
        0.0,
    )
    rank = jnp.dot(named, before, preferred_element_type=f32)
    mine = rank == slot
    return jnp.where(mine, named, 0.0), jnp.where(mine, weighted, 0.0)


def cell_kernel(
    slots, spans, relative,
    tokens_hbm, gain_hbm, next_gain_hbm, wq_hbm, wk_hbm, wv_hbm, wi_hbm, wf_hbm, bias_hbm, mem_hbm, norm_hbm,
    max_hbm, wo_hbm, ids_hbm, weights_hbm,
    partial_ref, keys_ref, values_ref, keep_ref, norm_out, max_out, placing_ref, mixing_ref, tokens_ref,
    next_gain_ref,
    gain_ref, wq_ref, wk_ref, wv_ref, wi_ref, wf_ref, bias_ref, mem_ref, norm_ref, max_ref, wo_ref, ids_ref,
    weights_ref, sems,
):
    pairs = (
        (tokens_hbm, tokens_ref), (gain_hbm, gain_ref), (wi_hbm, wi_ref), (wf_hbm, wf_ref), (bias_hbm, bias_ref),
        (max_hbm, max_ref), (ids_hbm, ids_ref), (weights_hbm, weights_ref), (norm_hbm, norm_ref),
        (wk_hbm, wk_ref), (wq_hbm, wq_ref), (wv_hbm, wv_ref), (mem_hbm, mem_ref), (wo_hbm, wo_ref),
        (next_gain_hbm, next_gain_ref),
    )
    copies = [pltpu.make_async_copy(a, b, sems.at[i]) for i, (a, b) in enumerate(pairs)]
    for copy in copies:
        copy.start()
    head = lax.axis_index("tp")
    seq_count = tokens_ref.shape[0]
    head_dim = wq_ref.shape[1]
    for copy in copies[:9]:
        copy.wait()
    base = lax.axis_index("ep") if relative else 0
    placing, mixing = routing(
        ids_ref[...], weights_ref[...], placing_ref.shape[0], slots, spans, base
    )
    placing_ref[...] = placing.astype(bf16)
    mixing_ref[...] = mixing
    normed = scaled_tiles(tokens_ref[...].astype(f32), gain_ref)

    def project(ref):
        return jnp.dot(normed, ref[...], preferred_element_type=f32).astype(bf16).astype(f32)

    def gate(ref):
        return lax.dot_general(
            normed, ref[...], (((1,), (1,)), ((), ())), preferred_element_type=f32
        )

    inputs = gate(wi_ref)
    forgets = gate(wf_ref) + bias_ref[...]
    here = lax.broadcasted_iota(jnp.int32, inputs.shape, 1) == head
    input_gate = jnp.sum(jnp.where(here, inputs, 0.0), 1, keepdims=True)
    forget = jnp.sum(jnp.where(here, forgets, 0.0), 1, keepdims=True)
    forget_log = jnp.minimum(forget, 0.0) - jnp.log1p(jnp.exp(-jnp.abs(forget)))
    held = forget_log + to_column(max_ref[...])
    new_max = jnp.maximum(held, input_gate)
    keep = jnp.exp(held - new_max)
    fresh = jnp.exp(input_gate - new_max)
    max_out[...] = to_row(new_max)
    keep_ref[...] = jnp.broadcast_to(keep, keep_ref.shape)
    for copy in copies[9:13]:
        copy.wait()
    key, query, value = project(wk_ref) * head_dim ** (-0.5), project(wq_ref), project(wv_ref)
    new_norm = keep * norm_ref[...] + fresh * key
    norm_out[...] = new_norm
    keys_ref[...] = fresh * key
    values_ref[...] = value
    query_t = query.T
    read = []
    for s in range(seq_count):
        read.append(jnp.sum(mem_ref[s] * query_t[:, s : s + 1], 0, keepdims=True))
    read = jnp.concatenate(read, 0)
    match = jnp.sum(query * key, 1, keepdims=True)
    numerator = keep * read + (fresh * match) * value
    denominator = jnp.sum(query * new_norm, 1, keepdims=True)
    readout = numerator / jnp.maximum(jnp.abs(denominator), jnp.exp(-new_max))
    for copy in copies[13:]:
        copy.wait()
    partial_ref[...] = jnp.dot(
        readout.astype(bf16), wo_ref[...], preferred_element_type=f32
    ).astype(bf16)


def pack_kernel(groups, tick_ref, tokens_ref, gain_ref, placing_ref, *refs):
    partials, outs, residual_ref = refs[: -groups - 1], refs[-groups - 1 : -1], refs[-1]
    total = partials[0][...].astype(f32)
    for ref in partials[1:]:
        total = total + ref[...].astype(f32)
    residual = (tokens_ref[...].astype(f32) + total).astype(bf16)
    residual_ref[...] = residual
    normed = scaled_tiles(residual.astype(f32), gain_ref)
    rows = jnp.dot(placing_ref[...], normed, preferred_element_type=f32)
    spread(rows, outs)


def spread(rows, outs):
    slots = outs[0].shape[1]
    for at in range(rows.shape[0] // slots):
        outs[at % len(outs)][at // len(outs)] = rows[at * slots : (at + 1) * slots, :].astype(bf16)


def join_kernel(tick_ref, near_ref, far_ref, *outs):
    for at, out_ref in enumerate(outs):
        out_ref[0] = near_ref[at]
        out_ref[1] = far_ref[at]


def fetch_kernel(tick_ref, source_ref, target_ref, sems):
    pieces = sems.shape[0]
    height = source_ref.shape[0] // pieces
    copies = []
    for at in range(pieces):
        rows = pl.ds(at * height, height)
        copies.append(
            pltpu.make_async_copy(source_ref.at[rows], target_ref.at[rows], sems.at[at])
        )
    for copy in copies:
        copy.start()
    for copy in copies:
        copy.wait()


def fetched(weight, after):
    return kernel_call(
        fetch_kernel,
        (pltpu.VMEM(weight.shape, weight.dtype),),
        (after, *in_hbm(weight)),
        in_specs=[ANY] * 2,
        out_specs=(ANY,),
        scratch=[pltpu.SemaphoreType.DMA((8,))],
        cost=20_000_000,
        limit=1 << 20,
    )[0]


def stacked(refs):
    return jnp.concatenate(
        [ref[at].astype(f32) for ref in refs for at in range(ref.shape[0])], 0
    )


def expert_kernel(*refs):
    *parts, gate_ref, up_ref, out_ref = refs
    rows = stacked(parts).astype(bf16)
    width = out_ref.shape[1]
    step = min(width, 256)
    for at in range(0, width, step):
        gate_sum = jnp.dot(rows, gate_ref[:, at : at + step], preferred_element_type=f32)
        up_sum = jnp.dot(rows, up_ref[:, at : at + step], preferred_element_type=f32)
        out_ref[:, at : at + step] = (gate_sum * jax.nn.sigmoid(gate_sum) * up_sum).astype(bf16)


def down_kernel(tp_count, *refs):
    hiddens, weight_ref, outs = refs[:tp_count], refs[tp_count], refs[tp_count + 1 :]
    me = lax.axis_index("tp")
    units = hiddens[0].shape[1]
    total = None
    for k in range(tp_count):
        start = pl.multiple_of((me ^ k) * units, units)
        term = jnp.dot(
            hiddens[k][...], weight_ref[pl.ds(start, units), :], preferred_element_type=f32
        )
        total = term if total is None else total + term
    spread(total, outs)


def state_kernel(tick_ref, mem_ref, keys_ref, values_ref, keep_ref, norm_ref, max_ref, out_ref, norm_out, max_out):
    norm_out[...] = norm_ref[...]
    max_out[...] = max_ref[...]
    keys_t = keys_ref[...].T
    value = values_ref[...]
    for s in range(mem_ref.shape[0]):
        out_ref[s] = (
            keep_ref[s : s + 1, :] * mem_ref[s] + keys_t[:, s : s + 1] * value[s : s + 1, :]
        )


def final_kernel(residual_ref, mixing_ref, *refs):
    *parts, out_ref = refs
    width = out_ref.shape[1]
    start = pl.multiple_of(lax.axis_index("tp") * width, width)
    routed = lax.dot_general(
        mixing_ref[...],
        stacked(parts),
        (((0,), (0,)), ((), ())),
        precision=lax.Precision.HIGHEST,
        preferred_element_type=f32,
    )
    out_ref[...] = (residual_ref[:, pl.ds(start, width)].astype(f32) + routed).astype(bf16)


def in_hbm(*values):
    return [pltpu.with_memory_space_constraint(value, pltpu.HBM) for value in values]


def swapped(value, axis, bits):
    count = lax.axis_size(axis)
    return lax.ppermute(value, axis, [(at, at ^ bits) for at in range(count)])


def from_partners(value, count):
    return [value] + [swapped(value, "tp", k) for k in range(1, count)]


def exchanged(near, far, meanwhile):
    came = swapped(far, "ep", 1)
    first = meanwhile[0](far)
    count, *block = near.shape
    joined = kernel_call(
        join_kernel,
        tuple(pltpu.VMEM((2, *block), near.dtype) for _ in range(count)),
        (came if first is None else first, near, came),
        in_specs=[ANY, VMEM, VMEM],
        limit=4 << 20,
    )
    parts = [joined[0]] + [swapped(joined[k], "ep", 2 * k) for k in range(1, count)]
    return parts, first, meanwhile[1](joined[1])


def shards(
    tokens, mix_gain, w_query, w_key, w_value, w_igate, w_fgate, forget_bias, w_out, mem_state, norm_state,
    max_state, ffn_gain, route_ids, route_weights, w_gate, w_up, w_down,
):
    seq_count, model_width = tokens.shape
    head_dim = norm_state.shape[1]
    tp_count = lax.axis_size("tp")
    ep_count = lax.axis_size("ep")
    own_width = model_width // tp_count
    top_count = route_ids.shape[1]
    spans = FF // w_down.shape[0]
    experts = ep_count // spans
    bound = max(2, 3 * seq_count * top_count // (2 * experts))
    slots = bound + bound % 2
    rows = ep_count * slots
    struct = jax.ShapeDtypeStruct
    direct = ep_count <= 8
    groups = 2 if direct else 1

    def block_outs(width):
        if direct:
            return tuple(pltpu.VMEM((ep_count // 2, slots, width), bf16) for _ in range(2))
        return (struct((ep_count, slots, width), bf16),)

    def delivered(blocks, *meanwhile):
        if direct:
            return exchanged(*blocks, meanwhile)
        moved = lax.all_to_all(blocks[0], "ep", split_axis=0, concat_axis=0, tiled=True)
        return [moved], *(work(blocks[0]) for work in meanwhile)


    memory = mem_state.reshape(seq_count, head_dim, head_dim)
    gain_shape = (model_width // LANES, LANES)
    sources = (
        tokens, mix_gain.reshape(gain_shape), ffn_gain.reshape(gain_shape), w_query, w_key, w_value, w_igate.T,
        w_fgate.T, forget_bias.reshape(1, -1), memory, norm_state, max_state.T, w_out, route_ids.T,
        route_weights.T,
    )
    partial, keys, values, keep, new_norm, new_max, placing, mixing, rows_in, gain_b = kernel_call(
        functools.partial(cell_kernel, slots, spans, direct),
        (
            pltpu.VMEM((seq_count, model_width), bf16),
            pltpu.VMEM((seq_count, head_dim), f32),
            pltpu.VMEM((seq_count, head_dim), f32),
            pltpu.VMEM((seq_count, head_dim), f32),
            pltpu.VMEM((seq_count, head_dim), f32),
            pltpu.VMEM((1, seq_count), f32),
            pltpu.VMEM((rows, seq_count), bf16),
            pltpu.VMEM((rows, seq_count), f32),
            pltpu.VMEM((seq_count, model_width), bf16),
            pltpu.VMEM(gain_shape, bf16),
        ),
        in_hbm(*sources),
        in_specs=[ANY] * len(sources),
        scratch=[
            *(pltpu.VMEM(v.shape, v.dtype) for v in (sources[1], *sources[3:])),
            pltpu.SemaphoreType.DMA((len(sources),)),
        ],
        limit=16 << 20,
    )
    partials = from_partners(partial, tp_count)
    gate_w = fetched(w_gate, partial)
    *blocks, residual = kernel_call(
        functools.partial(pack_kernel, groups),
        (*block_outs(model_width), pltpu.VMEM((seq_count, model_width), bf16)),
        (gate_w, rows_in, gain_b, placing, *partials),
        in_specs=[ANY] + [VMEM] * (3 + tp_count),
        limit=16 << 20,
    )
    arrived, up_w, down_w = delivered(
        blocks, functools.partial(fetched, w_up), functools.partial(fetched, w_down)
    )
    (hidden,) = kernel_call(
        expert_kernel,
        (pltpu.VMEM((rows, w_gate.shape[1]), bf16),),
        (*arrived, gate_w, up_w),
        limit=8 << 20,
    )
    hiddens = from_partners(hidden, tp_count)
    blocks = kernel_call(
        functools.partial(down_kernel, tp_count),
        block_outs(own_width),
        (*hiddens, down_w),
        limit=8 << 20,
    )

    def state(tick):
        return kernel_call(
            state_kernel,
            (
                struct((seq_count, head_dim, head_dim), f32),
                struct((seq_count, head_dim), f32),
                struct((1, seq_count), f32),
            ),
            (tick, memory, keys, values, keep, new_norm, new_max),
            in_specs=[ANY] + [VMEM] * 6,
            cost=20_000_000,
            limit=8 << 20,
        )

    returned, _, (new_memory, new_norm, new_max) = delivered(blocks, lambda tick: None, state)
    (out_tokens,) = kernel_call(
        final_kernel,
        (struct((seq_count, own_width), bf16),),
        (residual, mixing, *returned),
        limit=8 << 20,
    )
    return (
        out_tokens,
        new_memory.reshape(mem_state.shape),
        new_norm,
        new_max.T,
    )


def solution(mesh):
    placed = (
        P("ep", None),
        P(),
        P(None, "tp"),
        P(None, "tp"),
        P(None, "tp"),
        P(),
        P(),
        P(),
        P("tp", None),
        P("ep", "tp", None),
        P("ep", "tp"),
        P("ep", "tp"),
        P(),
        P("ep", None),
        P("ep", None),
        P(None, ("ep", "tp")),
        P(None, ("ep", "tp")),
        P("ep", "tp"),
    )
    return jax.shard_map(
        shards,
        mesh=mesh,
        in_specs=placed,
        out_specs=(P("ep", "tp"), P("ep", "tp", None), P("ep", "tp"), P("ep", "tp")),
        check_vma=False,
    )
```

```python
import functools
import jax
import jax.numpy as jnp
from jax import lax
from jax.experimental import pallas as pl
from jax.experimental.pallas import tpu as pltpu
from jax.sharding import PartitionSpec as P

FF = 4096
LANES = 128
epsilon = 1e-06
f32 = jnp.float32
bf16 = jnp.bfloat16


VMEM = pl.BlockSpec(memory_space=pltpu.VMEM)
ANY = pl.BlockSpec(memory_space=pl.ANY)


def kernel_call(body, outs, ins, in_specs=None, out_specs=None, scratch=(), cost=1000, limit=None):
    return pl.pallas_call(
        body,
        out_shape=outs,
        in_specs=in_specs or [VMEM] * len(ins),
        out_specs=out_specs or tuple([VMEM] * len(outs)),
        scratch_shapes=list(scratch),
        compiler_params=pltpu.CompilerParams(vmem_limit_bytes=limit),
        cost_estimate=pl.CostEstimate(flops=cost, bytes_accessed=0, transcendentals=0),
    )(*ins)


def scaled_tiles(wide, gain_ref):
    width = wide.shape[1]
    factor = lax.rsqrt(jnp.sum(wide * wide, 1, keepdims=True) / width + epsilon)
    gain = gain_ref[...].astype(f32)
    tiles = [
        wide[:, at * LANES : (at + 1) * LANES] * factor * gain[at : at + 1, :]
        for at in range(width // LANES)
    ]
    return jnp.concatenate(tiles, 1).astype(bf16)


def to_column(row):
    count = row.shape[1]
    eye = lax.broadcasted_iota(jnp.int32, (count, count), 0) == lax.broadcasted_iota(
        jnp.int32, (count, count), 1
    )
    return jnp.sum(jnp.where(eye, jnp.broadcast_to(row, (count, count)), 0.0), 1, keepdims=True)


def to_row(column):
    count = column.shape[0]
    eye = lax.broadcasted_iota(jnp.int32, (count, count), 0) == lax.broadcasted_iota(
        jnp.int32, (count, count), 1
    )
    return jnp.sum(jnp.where(eye, jnp.broadcast_to(column, (count, count)), 0.0), 0, keepdims=True)


def routing(ids, weights, rows, slots, spans, base, paired=0):
    top_count, seq_count = ids.shape
    at = lax.broadcasted_iota(jnp.int32, (rows, seq_count), 0)
    if paired:
        slot = (at // paired % slots).astype(f32)
        block = at % paired * 2 + at // (paired * slots)
    else:
        slot = (at % slots).astype(f32)
        block = at // slots
    expert = (block ^ base) // spans
    named = jnp.zeros((rows, seq_count), f32)
    weighted = jnp.zeros((rows, seq_count), f32)
    for k in range(top_count):
        hit = expert == ids[k : k + 1, :]
        named = named + jnp.where(hit, 1.0, 0.0)
        weighted = weighted + jnp.where(hit, weights[k : k + 1, :], 0.0)
    before = jnp.where(
        lax.broadcasted_iota(jnp.int32, (seq_count, seq_count), 0)
        < lax.broadcasted_iota(jnp.int32, (seq_count, seq_count), 1),
        1.0,
        0.0,
    )
    rank = jnp.dot(named, before, preferred_element_type=f32)
    mine = rank == slot
    return jnp.where(mine, named, 0.0), jnp.where(mine, weighted, 0.0)


def cell_kernel(
    slots, spans, paired,
    tokens_hbm, gain_hbm, next_gain_hbm, wq_hbm, wk_hbm, wv_hbm, wi_hbm, wf_hbm, bias_hbm, mem_hbm, norm_hbm,
    max_hbm, wo_hbm, ids_hbm, weights_hbm,
    partial_ref, keys_ref, values_ref, keep_ref, norm_out, max_out, placing_ref, mixing_ref, tokens_ref,
    next_gain_ref,
    gain_ref, wq_ref, wk_ref, wv_ref, wi_ref, wf_ref, bias_ref, mem_ref, norm_ref, max_ref, wo_ref, ids_ref,
    weights_ref, sems,
):
    pairs = (
        (tokens_hbm, tokens_ref), (gain_hbm, gain_ref), (ids_hbm, ids_ref), (weights_hbm, weights_ref),
        (wi_hbm, wi_ref), (wf_hbm, wf_ref), (bias_hbm, bias_ref), (max_hbm, max_ref), (norm_hbm, norm_ref),
        (wk_hbm, wk_ref), (wq_hbm, wq_ref), (mem_hbm, mem_ref), (wv_hbm, wv_ref), (wo_hbm, wo_ref),
        (next_gain_hbm, next_gain_ref),
    )
    copies = [pltpu.make_async_copy(a, b, sems.at[i]) for i, (a, b) in enumerate(pairs)]
    for copy in copies:
        copy.start()

    def arrive(first, last):
        for copy in copies[first:last]:
            copy.wait()

    head = lax.axis_index("tp")
    seq_count = tokens_ref.shape[0]
    head_dim = wq_ref.shape[1]
    arrive(0, 2)
    normed = scaled_tiles(tokens_ref[...].astype(f32), gain_ref)

    def project(ref):
        return jnp.dot(normed, ref[...], preferred_element_type=f32).astype(bf16).astype(f32)

    def gate(ref):
        return lax.dot_general(
            normed, ref[...], (((1,), (1,)), ((), ())), preferred_element_type=f32
        )

    arrive(2, 9)
    base = lax.axis_index("ep") if paired else 0
    shape = ids_ref[...], weights_ref[...], mixing_ref.shape[0], slots, spans, base
    placing, mixing = routing(*shape)
    if paired:
        placing, _ = routing(*shape, paired)
    placing_ref[...] = placing.astype(bf16)
    mixing_ref[...] = mixing
    inputs = gate(wi_ref)
    forgets = gate(wf_ref) + bias_ref[...]
    here = lax.broadcasted_iota(jnp.int32, inputs.shape, 1) == head
    input_gate = jnp.sum(jnp.where(here, inputs, 0.0), 1, keepdims=True)
    forget = jnp.sum(jnp.where(here, forgets, 0.0), 1, keepdims=True)
    forget_log = jnp.minimum(forget, 0.0) - jnp.log1p(jnp.exp(-jnp.abs(forget)))
    held = forget_log + to_column(max_ref[...])
    new_max = jnp.maximum(held, input_gate)
    keep = jnp.exp(held - new_max)
    fresh = jnp.exp(input_gate - new_max)
    max_out[...] = to_row(new_max)
    keep_ref[...] = jnp.broadcast_to(keep, keep_ref.shape)
    arrive(9, 10)
    key = project(wk_ref) * head_dim ** (-0.5)
    arrive(10, 11)
    query = project(wq_ref)
    query_t = query.T
    match = jnp.sum(query * key, 1, keepdims=True)
    new_norm = keep * norm_ref[...] + fresh * key
    norm_out[...] = new_norm
    keys_ref[...] = fresh * key
    denominator = jnp.sum(query * new_norm, 1, keepdims=True)
    scale = jnp.maximum(jnp.abs(denominator), jnp.exp(-new_max))
    arrive(11, 12)
    read = []
    for s in range(seq_count):
        read.append(jnp.sum(mem_ref[s] * query_t[:, s : s + 1], 0, keepdims=True))
    read = jnp.concatenate(read, 0)
    arrive(12, 13)
    value = project(wv_ref)
    values_ref[...] = value
    readout = (keep * read + (fresh * match) * value) / scale
    arrive(13, 14)
    partial_ref[...] = jnp.dot(
        readout.astype(bf16), wo_ref[...], preferred_element_type=f32
    ).astype(bf16)
    arrive(14, 15)


def pack_kernel(groups, tick_ref, tokens_ref, gain_ref, placing_ref, *refs):
    partials, outs, residual_ref = refs[: -groups - 1], refs[-groups - 1 : -1], refs[-1]
    total = partials[0][...].astype(f32)
    for ref in partials[1:]:
        total = total + ref[...].astype(f32)
    residual = (tokens_ref[...].astype(f32) + total).astype(bf16)
    residual_ref[...] = residual
    normed = scaled_tiles(residual.astype(f32), gain_ref)
    rows = jnp.dot(placing_ref[...], normed, preferred_element_type=f32).astype(bf16)
    if groups == 1:
        spread(rows, outs[0])
        return
    count, width = outs[0].shape[0], rows.shape[1]
    slots = outs[0].shape[1] // width
    for g, out_ref in enumerate(outs):
        for c in range(slots):
            start = (g * slots + c) * count
            out_ref[:, c * width : (c + 1) * width] = rows[start : start + count, :]


def spread(rows, out_ref):
    slots = out_ref.shape[1]
    for at in range(out_ref.shape[0]):
        out_ref[at] = rows[at * slots : (at + 1) * slots, :].astype(bf16)


def join_kernel(near_ref, far_ref, *outs):
    for at, out_ref in enumerate(outs):
        out_ref[0] = near_ref[at]
        out_ref[1] = far_ref[at]


def split_join_kernel(tick_ref, near_ref, far_ref, own_ref, first_ref, second_ref):
    near, far = near_ref[...].astype(f32), far_ref[...].astype(f32)

    def pair(at):
        return jnp.concatenate([near[at : at + 1, :], far[at : at + 1, :]], 0)

    odd = lax.axis_index("tp") & 1 == 1
    own_ref[...] = pair(0).astype(bf16)
    first_ref[...] = jnp.where(odd, pair(3), pair(1)).astype(bf16)
    second_ref[...] = pair(2).astype(bf16)


def fetch_kernel(tick_ref, source_ref, target_ref, sems):
    pieces = sems.shape[0]
    height = source_ref.shape[0] // pieces
    copies = []
    for at in range(pieces):
        rows = pl.ds(at * height, height)
        copies.append(
            pltpu.make_async_copy(source_ref.at[rows], target_ref.at[rows], sems.at[at])
        )
    for copy in copies:
        copy.start()
    for copy in copies:
        copy.wait()


def fetched(weight, after):
    return kernel_call(
        fetch_kernel,
        (pltpu.VMEM(weight.shape, weight.dtype),),
        (after, *in_hbm(weight)),
        in_specs=[ANY] * 2,
        out_specs=(ANY,),
        scratch=[pltpu.SemaphoreType.DMA((8,))],
        cost=20_000_000,
        limit=1 << 20,
    )[0]


def stacked(refs):
    return jnp.concatenate(
        [ref[at].astype(f32) for ref in refs for at in range(ref.shape[0])], 0
    )


def expert_kernel(*refs):
    *parts, gate_ref, up_ref, out_ref = refs
    deep = gate_ref.shape[0]
    if len(parts) == 1:
        rows = stacked(parts).astype(bf16)
    else:
        own, first, second, other_first, other_second = [ref[...].astype(f32) for ref in parts]
        odd = lax.axis_index("tp") & 1 == 1
        pieces = []
        for part in (
            own,
            jnp.where(odd, other_first, first),
            jnp.where(odd, second, other_second),
            jnp.where(odd, first, other_first),
        ):
            pieces += [part[:, at : at + deep] for at in range(0, part.shape[1], deep)]
        rows = jnp.concatenate(pieces, 0).astype(bf16)
    width = out_ref.shape[1]
    step = min(width, 512)
    for at in range(0, width, step):
        gate_sum = jnp.dot(rows, gate_ref[:, at : at + step], preferred_element_type=f32)
        up_sum = jnp.dot(rows, up_ref[:, at : at + step], preferred_element_type=f32)
        out_ref[:, at : at + step] = (gate_sum * jax.nn.sigmoid(gate_sum) * up_sum).astype(bf16)


def down_term(hidden_ref, weight_ref, k):
    units = hidden_ref.shape[1]
    start = pl.multiple_of((lax.axis_index("tp") ^ k) * units, units)
    return jnp.dot(
        hidden_ref[...], weight_ref[pl.ds(start, units), :], preferred_element_type=f32
    )


def first_down_kernel(near_ref, weight_ref, total_ref):
    total_ref[...] = down_term(near_ref, weight_ref, 0)


def down_kernel(tp_count, total_ref, *refs):
    hiddens, weight_ref, outs = refs[: tp_count - 1], refs[tp_count - 1], refs[tp_count:]
    total = total_ref[...]
    for k, hidden_ref in enumerate(hiddens):
        total = total + down_term(hidden_ref, weight_ref, 1 + k)
    if len(outs) == 1:
        spread(total, outs[0])
        return
    slots, count = outs[0].shape[1], len(outs)
    for g, out_ref in enumerate(outs):
        for at in range(out_ref.shape[0]):
            picked = [(at * slots + c) * count + g for c in range(slots)]
            out_ref[at] = jnp.concatenate([total[r : r + 1, :] for r in picked], 0).astype(bf16)


def state_kernel(tick_ref, mem_ref, keys_ref, values_ref, keep_ref, norm_ref, max_ref, out_ref, norm_out, max_out):
    norm_out[...] = norm_ref[...]
    max_out[...] = max_ref[...]
    keys_t = keys_ref[...].T
    value = values_ref[...]
    for s in range(mem_ref.shape[0]):
        out_ref[s] = (
            keep_ref[s : s + 1, :] * mem_ref[s] + keys_t[:, s : s + 1] * value[s : s + 1, :]
        )


def final_kernel(residual_ref, mixing_ref, *refs):
    *parts, out_ref = refs
    width = out_ref.shape[1]
    start = pl.multiple_of(lax.axis_index("tp") * width, width)
    routed = lax.dot_general(
        mixing_ref[...],
        stacked(parts),
        (((0,), (0,)), ((), ())),
        precision=lax.Precision.HIGHEST,
        preferred_element_type=f32,
    )
    out_ref[...] = (residual_ref[:, pl.ds(start, width)].astype(f32) + routed).astype(bf16)


def in_hbm(*values):
    return [pltpu.with_memory_space_constraint(value, pltpu.HBM) for value in values]


def swapped(value, axis, bits):
    count = lax.axis_size(axis)
    return lax.ppermute(value, axis, [(at, at ^ bits) for at in range(count)])


def sent(value, target):
    ep_count, tp_count = lax.axis_size("ep"), lax.axis_size("tp")
    pairs = []
    for e in range(ep_count):
        for t in range(tp_count):
            to_e, to_t = target(e, t)
            pairs.append((e * tp_count + t, to_e * tp_count + to_t))
    return lax.ppermute(value, ("ep", "tp"), pairs)


def from_partners(value, count):
    moved = [swapped(value, "tp", k) for k in reversed(range(1, count))]
    return [value, *reversed(moved)]


def gathered(near, far, w_up):
    came = swapped(far, "ep", 1)
    up_w = fetched(w_up, far)
    pair = (2, near.shape[1])
    own, first, second = kernel_call(
        split_join_kernel,
        tuple(pltpu.VMEM(pair, near.dtype) for _ in range(3)),
        (up_w, near, came),
        in_specs=[ANY, VMEM, VMEM],
        limit=4 << 20,
    )
    first = sent(first, lambda e, t: (e ^ 6, t) if t & 1 else (e ^ 2, t))
    second = sent(second, lambda e, t: (e ^ 4, t) if t & 1 else (e, t ^ 2))
    shared = [swapped(part, "tp", 1) for part in (first, second)]
    return [own, first, second, *shared], up_w


def returned_blocks(near, far):
    came = swapped(far, "ep", 1)
    count, *block = near.shape
    joined = kernel_call(
        join_kernel,
        tuple(pltpu.VMEM((2, *block), near.dtype) for _ in range(count)),
        (near, came),
        limit=4 << 20,
    )
    moved = [swapped(joined[k], "ep", 2 * k) for k in reversed(range(1, count))]
    return [joined[0], *reversed(moved)], joined[1]


def shards(
    tokens, mix_gain, w_query, w_key, w_value, w_igate, w_fgate, forget_bias, w_out, mem_state, norm_state,
    max_state, ffn_gain, route_ids, route_weights, w_gate, w_up, w_down,
):
    seq_count, model_width = tokens.shape
    head_dim = norm_state.shape[1]
    tp_count = lax.axis_size("tp")
    ep_count = lax.axis_size("ep")
    own_width = model_width // tp_count
    top_count = route_ids.shape[1]
    spans = FF // w_down.shape[0]
    experts = ep_count // spans
    bound = max(2, 3 * seq_count * top_count // (2 * experts))
    slots = bound
    rows = ep_count * slots
    struct = jax.ShapeDtypeStruct
    direct = ep_count <= 8
    groups = 2 if direct else 1

    def block_outs(width):
        if direct:
            return tuple(pltpu.VMEM((ep_count // 2, slots, width), bf16) for _ in range(2))
        return (struct((ep_count, slots, width), bf16),)

    memory = mem_state.reshape(seq_count, head_dim, head_dim)
    gain_shape = (model_width // LANES, LANES)
    sources = (
        tokens, mix_gain.reshape(gain_shape), ffn_gain.reshape(gain_shape), w_query, w_key, w_value, w_igate.T,
        w_fgate.T, forget_bias.reshape(1, -1), memory, norm_state, max_state.T, w_out, route_ids.T,
        route_weights.T,
    )
    partial, keys, values, keep, new_norm, new_max, placing, mixing, rows_in, gain_b = kernel_call(
        functools.partial(cell_kernel, slots, spans, ep_count // 2 if direct else 0),
        (
            pltpu.VMEM((seq_count, model_width), bf16),
            pltpu.VMEM((seq_count, head_dim), f32),
            pltpu.VMEM((seq_count, head_dim), f32),
            pltpu.VMEM((seq_count, head_dim), f32),
            pltpu.VMEM((seq_count, head_dim), f32),
            pltpu.VMEM((1, seq_count), f32),
            pltpu.VMEM((rows, seq_count), bf16),
            pltpu.VMEM((rows, seq_count), f32),
            pltpu.VMEM((seq_count, model_width), bf16),
            pltpu.VMEM(gain_shape, bf16),
        ),
        in_hbm(*sources),
        in_specs=[ANY] * len(sources),
        scratch=[
            *(pltpu.VMEM(v.shape, v.dtype) for v in (sources[1], *sources[3:])),
            pltpu.SemaphoreType.DMA((len(sources),)),
        ],
        limit=16 << 20,
    )
    partials = from_partners(partial, tp_count)
    gate_w = fetched(w_gate, partial)
    if direct:
        packed_outs = [pltpu.VMEM((ep_count // 2, slots * model_width), bf16) for _ in range(2)]
    else:
        packed_outs = block_outs(model_width)
    *blocks, residual = kernel_call(
        functools.partial(pack_kernel, groups),
        (*packed_outs, pltpu.VMEM((seq_count, model_width), bf16)),
        (gate_w, rows_in, gain_b, placing, *partials),
        in_specs=[ANY] + [VMEM] * (3 + tp_count),
        limit=16 << 20,
    )
    if direct:
        arrived, up_w = gathered(*blocks, w_up)
    else:
        arrived = [lax.all_to_all(blocks[0], "ep", split_axis=0, concat_axis=0, tiled=True)]
        up_w = fetched(w_up, blocks[0])
    (hidden,) = kernel_call(
        expert_kernel,
        (pltpu.VMEM((rows, w_gate.shape[1]), bf16),),
        (*arrived, gate_w, up_w),
        limit=8 << 20,
    )
    hiddens = from_partners(hidden, tp_count)
    down_w = fetched(w_down, hidden)
    (total,) = kernel_call(
        first_down_kernel,
        (pltpu.VMEM((rows, own_width), f32),),
        (hidden, down_w),
        cost=2_000_000,
        limit=8 << 20,
    )
    blocks = kernel_call(
        functools.partial(down_kernel, tp_count),
        block_outs(own_width),
        (total, *hiddens[1:], down_w),
        limit=8 << 20,
    )

    def state(tick):
        return kernel_call(
            state_kernel,
            (
                struct((seq_count, head_dim, head_dim), f32),
                struct((seq_count, head_dim), f32),
                struct((1, seq_count), f32),
            ),
            (tick, memory, keys, values, keep, new_norm, new_max),
            in_specs=[ANY] + [VMEM] * 6,
            cost=20_000_000,
            limit=8 << 20,
        )

    if direct:
        returned, tick = returned_blocks(*blocks)
    else:
        tick = blocks[0]
        returned = [lax.all_to_all(tick, "ep", split_axis=0, concat_axis=0, tiled=True)]
    new_memory, new_norm, new_max = state(tick)
    (out_tokens,) = kernel_call(
        final_kernel,
        (struct((seq_count, own_width), bf16),),
        (residual, mixing, *returned),
        limit=8 << 20,
    )
    return (
        out_tokens,
        new_memory.reshape(mem_state.shape),
        new_norm,
        new_max.T,
    )


def solution(mesh):
    placed = (
        P("ep", None),
        P(),
        P(None, "tp"),
        P(None, "tp"),
        P(None, "tp"),
        P(),
        P(),
        P(),
        P("tp", None),
        P("ep", "tp", None),
        P("ep", "tp"),
        P("ep", "tp"),
        P(),
        P("ep", None),
        P("ep", None),
        P(None, ("ep", "tp")),
        P(None, ("ep", "tp")),
        P("ep", "tp"),
    )

    return jax.shard_map(
        shards,
        mesh=mesh,
        in_specs=placed,
        out_specs=(P("ep", "tp"), P("ep", "tp", None), P("ep", "tp"), P("ep", "tp")),
        check_vma=False,
    )
```

```python
import functools
import jax
import jax.numpy as jnp
from jax import lax
from jax.experimental import pallas as pl
from jax.experimental.pallas import tpu as pltpu
from jax.sharding import PartitionSpec as P

FF = 4096
LATEST = 2
LANES = 128
epsilon = 1e-06
f32 = jnp.float32
bf16 = jnp.bfloat16


VMEM = pl.BlockSpec(memory_space=pltpu.VMEM)
ANY = pl.BlockSpec(memory_space=pl.ANY)


def kernel_call(body, outs, ins, in_specs=None, out_specs=None, scratch=(), cost=1000, limit=None):
    return pl.pallas_call(
        body,
        out_shape=outs,
        in_specs=in_specs or [VMEM] * len(ins),
        out_specs=out_specs or tuple([VMEM] * len(outs)),
        scratch_shapes=list(scratch),
        compiler_params=pltpu.CompilerParams(vmem_limit_bytes=limit),
        cost_estimate=pl.CostEstimate(flops=cost, bytes_accessed=0, transcendentals=0),
    )(*ins)


def scaled_tiles(wide, gain_ref):
    width = wide.shape[1]
    factor = lax.rsqrt(jnp.sum(wide * wide, 1, keepdims=True) / width + epsilon)
    gain = gain_ref[...].astype(f32)
    tiles = [
        wide[:, at * LANES : (at + 1) * LANES] * factor * gain[at : at + 1, :]
        for at in range(width // LANES)
    ]
    return jnp.concatenate(tiles, 1).astype(bf16)


def to_column(row):
    count = row.shape[1]
    eye = lax.broadcasted_iota(jnp.int32, (count, count), 0) == lax.broadcasted_iota(
        jnp.int32, (count, count), 1
    )
    return jnp.sum(jnp.where(eye, jnp.broadcast_to(row, (count, count)), 0.0), 1, keepdims=True)


def to_row(column):
    count = column.shape[0]
    eye = lax.broadcasted_iota(jnp.int32, (count, count), 0) == lax.broadcasted_iota(
        jnp.int32, (count, count), 1
    )
    return jnp.sum(jnp.where(eye, jnp.broadcast_to(column, (count, count)), 0.0), 0, keepdims=True)


def routing(ids, weights, rows, slots, spans, base, paired=0):
    top_count, seq_count = ids.shape
    at = lax.broadcasted_iota(jnp.int32, (rows, seq_count), 0)
    if paired:
        slot = (at // paired % slots).astype(f32)
        block = at % paired * 2 + at // (paired * slots)
    else:
        slot = (at % slots).astype(f32)
        block = at // slots
    expert = (block ^ base) // spans
    named = jnp.zeros((rows, seq_count), f32)
    weighted = jnp.zeros((rows, seq_count), f32)
    for k in range(top_count):
        hit = expert == ids[k : k + 1, :]
        named = named + jnp.where(hit, 1.0, 0.0)
        weighted = weighted + jnp.where(hit, weights[k : k + 1, :], 0.0)
    before = jnp.where(
        lax.broadcasted_iota(jnp.int32, (seq_count, seq_count), 0)
        < lax.broadcasted_iota(jnp.int32, (seq_count, seq_count), 1),
        1.0,
        0.0,
    )
    rank = jnp.dot(named, before, preferred_element_type=f32)
    mine = rank == slot
    return jnp.where(mine, named, 0.0), jnp.where(mine, weighted, 0.0)


def cell_kernel(
    slots, spans, paired,
    tokens_hbm, gain_hbm, next_gain_hbm, wq_hbm, wk_hbm, wv_hbm, wi_hbm, wf_hbm, bias_hbm, mem_hbm, norm_hbm,
    max_hbm, wo_hbm, ids_hbm, weights_hbm,
    partial_ref, keys_ref, values_ref, keep_ref, norm_out, max_out, placing_ref, mixing_ref, tokens_ref,
    next_gain_ref,
    gain_ref, wq_ref, wk_ref, wv_ref, wi_ref, wf_ref, bias_ref, mem_ref, norm_ref, max_ref, wo_ref, ids_ref,
    weights_ref, sems,
):
    pairs = (
        (tokens_hbm, tokens_ref), (gain_hbm, gain_ref), (ids_hbm, ids_ref), (weights_hbm, weights_ref),
        (wi_hbm, wi_ref), (wf_hbm, wf_ref), (bias_hbm, bias_ref), (max_hbm, max_ref), (norm_hbm, norm_ref),
        (wk_hbm, wk_ref), (wq_hbm, wq_ref), (mem_hbm, mem_ref), (wv_hbm, wv_ref), (wo_hbm, wo_ref),
        (next_gain_hbm, next_gain_ref),
    )
    copies = [pltpu.make_async_copy(a, b, sems.at[i]) for i, (a, b) in enumerate(pairs)]
    for copy in copies:
        copy.start()

    def arrive(first, last):
        for copy in copies[first:last]:
            copy.wait()

    head = lax.axis_index("tp")
    seq_count = tokens_ref.shape[0]
    head_dim = wq_ref.shape[1]
    arrive(0, 2)
    normed = scaled_tiles(tokens_ref[...].astype(f32), gain_ref)

    def project(ref):
        return jnp.dot(normed, ref[...], preferred_element_type=f32).astype(bf16).astype(f32)

    def gate(ref):
        return lax.dot_general(
            normed, ref[...], (((1,), (1,)), ((), ())), preferred_element_type=f32
        )

    arrive(2, 9)
    base = lax.axis_index("ep") if paired else 0
    shape = ids_ref[...], weights_ref[...], mixing_ref.shape[0], slots, spans, base
    placing, mixing = routing(*shape)
    if paired:
        placing, _ = routing(*shape, paired)
    placing_ref[...] = placing.astype(bf16)
    mixing_ref[...] = mixing
    inputs = gate(wi_ref)
    forgets = gate(wf_ref) + bias_ref[...]
    here = lax.broadcasted_iota(jnp.int32, inputs.shape, 1) == head
    input_gate = jnp.sum(jnp.where(here, inputs, 0.0), 1, keepdims=True)
    forget = jnp.sum(jnp.where(here, forgets, 0.0), 1, keepdims=True)
    forget_log = jnp.minimum(forget, 0.0) - jnp.log1p(jnp.exp(-jnp.abs(forget)))
    held = forget_log + to_column(max_ref[...])
    new_max = jnp.maximum(held, input_gate)
    keep = jnp.exp(held - new_max)
    fresh = jnp.exp(input_gate - new_max)
    max_out[...] = to_row(new_max)
    keep_ref[...] = jnp.broadcast_to(keep, keep_ref.shape)
    arrive(9, 10)
    key = project(wk_ref) * head_dim ** (-0.5)
    arrive(10, 11)
    query = project(wq_ref)
    query_t = query.T
    match = jnp.sum(query * key, 1, keepdims=True)
    new_norm = keep * norm_ref[...] + fresh * key
    norm_out[...] = new_norm
    keys_ref[...] = fresh * key
    denominator = jnp.sum(query * new_norm, 1, keepdims=True)
    scale = jnp.maximum(jnp.abs(denominator), jnp.exp(-new_max))
    arrive(11, 12)
    read = []
    for s in range(seq_count):
        read.append(jnp.sum(mem_ref[s] * query_t[:, s : s + 1], 0, keepdims=True))
    read = jnp.concatenate(read, 0)
    arrive(12, 13)
    value = project(wv_ref)
    values_ref[...] = value
    readout = (keep * read + (fresh * match) * value) / scale
    arrive(13, 14)
    partial_ref[...] = jnp.dot(
        readout.astype(bf16), wo_ref[...], preferred_element_type=f32
    ).astype(bf16)
    arrive(14, 15)


def pack_kernel(groups, tick_ref, tokens_ref, gain_ref, placing_ref, *refs):
    partials, outs, residual_ref = refs[: -groups - 1], refs[-groups - 1 : -1], refs[-1]
    total = partials[0][...].astype(f32)
    for ref in partials[1:]:
        total = total + ref[...].astype(f32)
    residual = (tokens_ref[...].astype(f32) + total).astype(bf16)
    residual_ref[...] = residual
    normed = scaled_tiles(residual.astype(f32), gain_ref)
    rows = jnp.dot(placing_ref[...], normed, preferred_element_type=f32).astype(bf16)
    if groups == 1:
        spread(rows, outs[0])
        return
    count, width = outs[0].shape[0], rows.shape[1]
    slots = outs[0].shape[1] // width
    for g, out_ref in enumerate(outs):
        for c in range(slots):
            start = (g * slots + c) * count
            out_ref[:, c * width : (c + 1) * width] = rows[start : start + count, :]


def spread(rows, out_ref):
    slots = out_ref.shape[1]
    for at in range(out_ref.shape[0]):
        out_ref[at] = rows[at * slots : (at + 1) * slots, :].astype(bf16)


def join_kernel(near_ref, far_ref, *outs):
    for at, out_ref in enumerate(outs):
        out_ref[0] = near_ref[at]
        out_ref[1] = far_ref[at]


def split_join_kernel(tick_ref, near_ref, far_ref, own_ref, first_ref, second_ref):
    near, far = near_ref[...].astype(f32), far_ref[...].astype(f32)

    def pair(at):
        return jnp.concatenate([near[at : at + 1, :], far[at : at + 1, :]], 0)

    odd = lax.axis_index("tp") & 1 == 1
    own_ref[...] = pair(0).astype(bf16)
    first_ref[...] = jnp.where(odd, pair(3), pair(1)).astype(bf16)
    second_ref[...] = pair(2).astype(bf16)


def fetch_kernel(tick_ref, source_ref, target_ref, sems):
    pieces = sems.shape[0]
    height = source_ref.shape[0] // pieces
    copies = []
    for at in range(pieces):
        rows = pl.ds(at * height, height)
        copies.append(
            pltpu.make_async_copy(source_ref.at[rows], target_ref.at[rows], sems.at[at])
        )
    for copy in copies:
        copy.start()
    for copy in copies:
        copy.wait()


def fetched(weight, after):
    return kernel_call(
        fetch_kernel,
        (pltpu.VMEM(weight.shape, weight.dtype),),
        (after, *in_hbm(weight)),
        in_specs=[ANY] * 2,
        out_specs=(ANY,),
        scratch=[pltpu.SemaphoreType.DMA((8,))],
        cost=20_000_000,
        limit=1 << 20,
    )[0]


def stacked(refs):
    return jnp.concatenate(
        [ref[at].astype(f32) for ref in refs for at in range(ref.shape[0])], 0
    )


def expert_kernel(*refs):
    *parts, gate_ref, up_ref, out_ref = refs
    deep = gate_ref.shape[0]
    if len(parts) == 1:
        rows = stacked(parts).astype(bf16)
    else:
        own, first, second, other_first, other_second = [ref[...].astype(f32) for ref in parts]
        odd = lax.axis_index("tp") & 1 == 1
        pieces = []
        for part in (
            own,
            jnp.where(odd, other_first, first),
            jnp.where(odd, second, other_second),
            jnp.where(odd, first, other_first),
        ):
            pieces += [part[:, at : at + deep] for at in range(0, part.shape[1], deep)]
        rows = jnp.concatenate(pieces, 0).astype(bf16)
    width = out_ref.shape[1]
    step = min(width, 512)
    for at in range(0, width, step):
        gate_sum = jnp.dot(rows, gate_ref[:, at : at + step], preferred_element_type=f32)
        up_sum = jnp.dot(rows, up_ref[:, at : at + step], preferred_element_type=f32)
        out_ref[:, at : at + step] = (gate_sum * jax.nn.sigmoid(gate_sum) * up_sum).astype(bf16)


def down_term(hidden_ref, weight_ref, k):
    units = hidden_ref.shape[1]
    start = pl.multiple_of((lax.axis_index("tp") ^ k) * units, units)
    return jnp.dot(
        hidden_ref[...], weight_ref[pl.ds(start, units), :], preferred_element_type=f32
    )


def first_down_kernel(own_ref, weight_ref, total_ref):
    total_ref[...] = down_term(own_ref, weight_ref, 0)


def next_down_kernel(numbers, before_ref, *refs):
    *hiddens, weight_ref, total_ref = refs
    total = before_ref[...]
    for k, hidden_ref in zip(numbers, hiddens):
        total = total + down_term(hidden_ref, weight_ref, k)
    total_ref[...] = total


def down_kernel(total_ref, hidden_ref, weight_ref, *outs):
    total = total_ref[...] + down_term(hidden_ref, weight_ref, LATEST)
    if len(outs) == 1:
        spread(total, outs[0])
        return
    slots, count = outs[0].shape[1], len(outs)
    for g, out_ref in enumerate(outs):
        for at in range(out_ref.shape[0]):
            picked = [(at * slots + c) * count + g for c in range(slots)]
            out_ref[at] = jnp.concatenate([total[r : r + 1, :] for r in picked], 0).astype(bf16)


def state_kernel(tick_ref, mem_ref, keys_ref, values_ref, keep_ref, norm_ref, max_ref, out_ref, norm_out, max_out):
    norm_out[...] = norm_ref[...]
    max_out[...] = max_ref[...]
    keys_t = keys_ref[...].T
    value = values_ref[...]
    for s in range(mem_ref.shape[0]):
        out_ref[s] = (
            keep_ref[s : s + 1, :] * mem_ref[s] + keys_t[:, s : s + 1] * value[s : s + 1, :]
        )


def final_kernel(residual_ref, mixing_ref, *refs):
    *parts, out_ref = refs
    width = out_ref.shape[1]
    start = pl.multiple_of(lax.axis_index("tp") * width, width)
    weights = mixing_ref[...].T
    routed, at = None, 0
    for ref in parts:
        for place in range(ref.shape[0]):
            block = ref[place].astype(f32)
            for c in range(ref.shape[1]):
                term = weights[:, at : at + 1] * block[c : c + 1, :]
                routed = term if routed is None else routed + term
                at += 1
    out_ref[...] = (residual_ref[:, pl.ds(start, width)].astype(f32) + routed).astype(bf16)


def in_hbm(*values):
    return [pltpu.with_memory_space_constraint(value, pltpu.HBM) for value in values]


def swapped(value, axis, bits):
    count = lax.axis_size(axis)
    return lax.ppermute(value, axis, [(at, at ^ bits) for at in range(count)])


def sent(value, target):
    ep_count, tp_count = lax.axis_size("ep"), lax.axis_size("tp")
    pairs = []
    for e in range(ep_count):
        for t in range(tp_count):
            to_e, to_t = target(e, t)
            pairs.append((e * tp_count + t, to_e * tp_count + to_t))
    return lax.ppermute(value, ("ep", "tp"), pairs)


def from_partners(value, count):
    moved = [swapped(value, "tp", k) for k in reversed(range(1, count))]
    return [value, *reversed(moved)]


def gathered(near, far, w_up):
    came = swapped(far, "ep", 1)
    up_w = fetched(w_up, far)
    pair = (2, near.shape[1])
    own, first, second = kernel_call(
        split_join_kernel,
        tuple(pltpu.VMEM(pair, near.dtype) for _ in range(3)),
        (up_w, near, came),
        in_specs=[ANY, VMEM, VMEM],
        limit=4 << 20,
    )
    first = sent(first, lambda e, t: (e ^ 6, t) if t & 1 else (e ^ 2, t))
    second = sent(second, lambda e, t: (e ^ 4, t) if t & 1 else (e, t ^ 2))
    shared = [swapped(part, "tp", 1) for part in (first, second)]
    return [own, first, second, *shared], up_w


def returned_blocks(near, far):
    came = swapped(far, "ep", 1)
    count, *block = near.shape
    joined = kernel_call(
        join_kernel,
        tuple(pltpu.VMEM((2, *block), near.dtype) for _ in range(count)),
        (near, came),
        limit=4 << 20,
    )
    moved = [swapped(joined[k], "ep", 2 * k) for k in reversed(range(1, count))]
    return [joined[0], *reversed(moved)], joined[1]


def shards(
    tokens, mix_gain, w_query, w_key, w_value, w_igate, w_fgate, forget_bias, w_out, mem_state, norm_state,
    max_state, ffn_gain, route_ids, route_weights, w_gate, w_up, w_down,
):
    seq_count, model_width = tokens.shape
    head_dim = norm_state.shape[1]
    tp_count = lax.axis_size("tp")
    ep_count = lax.axis_size("ep")
    own_width = model_width // tp_count
    top_count = route_ids.shape[1]
    spans = FF // w_down.shape[0]
    experts = ep_count // spans
    bound = max(2, 3 * seq_count * top_count // (2 * experts))
    slots = bound
    rows = ep_count * slots
    struct = jax.ShapeDtypeStruct
    direct = ep_count <= 8
    groups = 2 if direct else 1

    def block_outs(width):
        if direct:
            return tuple(pltpu.VMEM((ep_count // 2, slots, width), bf16) for _ in range(2))
        return (struct((ep_count, slots, width), bf16),)

    memory = mem_state.reshape(seq_count, head_dim, head_dim)
    gain_shape = (model_width // LANES, LANES)
    sources = (
        tokens, mix_gain.reshape(gain_shape), ffn_gain.reshape(gain_shape), w_query, w_key, w_value, w_igate.T,
        w_fgate.T, forget_bias.reshape(1, -1), memory, norm_state, max_state.T, w_out, route_ids.T,
        route_weights.T,
    )
    partial, keys, values, keep, new_norm, new_max, placing, mixing, rows_in, gain_b = kernel_call(
        functools.partial(cell_kernel, slots, spans, ep_count // 2 if direct else 0),
        (
            pltpu.VMEM((seq_count, model_width), bf16),
            pltpu.VMEM((seq_count, head_dim), f32),
            pltpu.VMEM((seq_count, head_dim), f32),
            pltpu.VMEM((seq_count, head_dim), f32),
            pltpu.VMEM((seq_count, head_dim), f32),
            pltpu.VMEM((1, seq_count), f32),
            pltpu.VMEM((rows, seq_count), bf16),
            pltpu.VMEM((rows, seq_count), f32),
            pltpu.VMEM((seq_count, model_width), bf16),
            pltpu.VMEM(gain_shape, bf16),
        ),
        in_hbm(*sources),
        in_specs=[ANY] * len(sources),
        scratch=[
            *(pltpu.VMEM(v.shape, v.dtype) for v in (sources[1], *sources[3:])),
            pltpu.SemaphoreType.DMA((len(sources),)),
        ],
        limit=16 << 20,
    )
    partials = from_partners(partial, tp_count)
    gate_w = fetched(w_gate, partial)
    if direct:
        packed_outs = [pltpu.VMEM((ep_count // 2, slots * model_width), bf16) for _ in range(2)]
    else:
        packed_outs = block_outs(model_width)
    *blocks, residual = kernel_call(
        functools.partial(pack_kernel, groups),
        (*packed_outs, pltpu.VMEM((seq_count, model_width), bf16)),
        (gate_w, rows_in, gain_b, placing, *partials),
        in_specs=[ANY] + [VMEM] * (3 + tp_count),
        limit=16 << 20,
    )
    if direct:
        arrived, up_w = gathered(*blocks, w_up)
    else:
        arrived = [lax.all_to_all(blocks[0], "ep", split_axis=0, concat_axis=0, tiled=True)]
        up_w = fetched(w_up, blocks[0])
    (hidden,) = kernel_call(
        expert_kernel,
        (pltpu.VMEM((rows, w_gate.shape[1]), bf16),),
        (*arrived, gate_w, up_w),
        limit=8 << 20,
    )
    hiddens = from_partners(hidden, tp_count)
    down_w = fetched(w_down, hidden)
    (total,) = kernel_call(
        first_down_kernel,
        (pltpu.VMEM((rows, own_width), f32),),
        (hidden, down_w),
        cost=2_000_000,
        limit=8 << 20,
    )
    middle = [k for k in reversed(range(1, tp_count)) if k != LATEST]
    (total,) = kernel_call(
        functools.partial(next_down_kernel, middle),
        (pltpu.VMEM((rows, own_width), f32),),
        (total, *(hiddens[k] for k in middle), down_w),
        cost=2_000_000,
        limit=8 << 20,
    )
    blocks = kernel_call(
        down_kernel,
        block_outs(own_width),
        (total, hiddens[LATEST], down_w),
        limit=8 << 20,
    )

    def state(tick):
        return kernel_call(
            state_kernel,
            (
                struct((seq_count, head_dim, head_dim), f32),
                struct((seq_count, head_dim), f32),
                struct((1, seq_count), f32),
            ),
            (tick, memory, keys, values, keep, new_norm, new_max),
            in_specs=[ANY] + [VMEM] * 6,
            cost=20_000_000,
            limit=8 << 20,
        )

    if direct:
        returned, tick = returned_blocks(*blocks)
    else:
        tick = blocks[0]
        returned = [lax.all_to_all(tick, "ep", split_axis=0, concat_axis=0, tiled=True)]
    new_memory, new_norm, new_max = state(tick)
    (out_tokens,) = kernel_call(
        final_kernel,
        (struct((seq_count, own_width), bf16),),
        (residual, mixing, *returned),
        limit=8 << 20,
    )
    return (
        out_tokens,
        new_memory.reshape(mem_state.shape),
        new_norm,
        new_max.T,
    )


def solution(mesh):
    placed = (
        P("ep", None),
        P(),
        P(None, "tp"),
        P(None, "tp"),
        P(None, "tp"),
        P(),
        P(),
        P(),
        P("tp", None),
        P("ep", "tp", None),
        P("ep", "tp"),
        P("ep", "tp"),
        P(),
        P("ep", None),
        P("ep", None),
        P(None, ("ep", "tp")),
        P(None, ("ep", "tp")),
        P("ep", "tp"),
    )

    return jax.shard_map(
        shards,
        mesh=mesh,
        in_specs=placed,
        out_specs=(P("ep", "tp"), P("ep", "tp", None), P("ep", "tp"), P("ep", "tp")),
        check_vma=False,
    )
```

```python
import functools
import jax
import jax.numpy as jnp
from jax import lax
from jax.experimental import pallas as pl
from jax.experimental.pallas import tpu as pltpu
from jax.sharding import PartitionSpec as P

FF = 4096
LATEST = 2
LANES = 128
epsilon = 1e-06
f32 = jnp.float32
bf16 = jnp.bfloat16


VMEM = pl.BlockSpec(memory_space=pltpu.VMEM)
ANY = pl.BlockSpec(memory_space=pl.ANY)


def kernel_call(body, outs, ins, in_specs=None, out_specs=None, scratch=(), cost=1000, limit=None):
    return pl.pallas_call(
        body,
        out_shape=outs,
        in_specs=in_specs or [VMEM] * len(ins),
        out_specs=out_specs or tuple([VMEM] * len(outs)),
        scratch_shapes=list(scratch),
        compiler_params=pltpu.CompilerParams(vmem_limit_bytes=limit),
        cost_estimate=pl.CostEstimate(flops=cost, bytes_accessed=0, transcendentals=0),
    )(*ins)


def scaled_tiles(wide, gain_ref):
    width = wide.shape[1]
    factor = lax.rsqrt(jnp.sum(wide * wide, 1, keepdims=True) / width + epsilon)
    gain = gain_ref[...].astype(f32)
    tiles = [
        wide[:, at * LANES : (at + 1) * LANES] * factor * gain[at : at + 1, :]
        for at in range(width // LANES)
    ]
    return jnp.concatenate(tiles, 1).astype(bf16)


def to_column(row):
    count = row.shape[1]
    eye = lax.broadcasted_iota(jnp.int32, (count, count), 0) == lax.broadcasted_iota(
        jnp.int32, (count, count), 1
    )
    return jnp.sum(jnp.where(eye, jnp.broadcast_to(row, (count, count)), 0.0), 1, keepdims=True)


def to_row(column):
    count = column.shape[0]
    eye = lax.broadcasted_iota(jnp.int32, (count, count), 0) == lax.broadcasted_iota(
        jnp.int32, (count, count), 1
    )
    return jnp.sum(jnp.where(eye, jnp.broadcast_to(column, (count, count)), 0.0), 0, keepdims=True)


def routing(ids, weights, rows, slots, spans, base, paired=0):
    top_count, seq_count = ids.shape
    at = lax.broadcasted_iota(jnp.int32, (rows, seq_count), 0)
    if paired:
        slot = (at // paired % slots).astype(f32)
        block = at % paired * 2 + at // (paired * slots)
    else:
        slot = (at % slots).astype(f32)
        block = at // slots
    expert = (block ^ base) // spans
    named = jnp.zeros((rows, seq_count), f32)
    weighted = jnp.zeros((rows, seq_count), f32)
    for k in range(top_count):
        hit = expert == ids[k : k + 1, :]
        named = named + jnp.where(hit, 1.0, 0.0)
        weighted = weighted + jnp.where(hit, weights[k : k + 1, :], 0.0)
    before = jnp.where(
        lax.broadcasted_iota(jnp.int32, (seq_count, seq_count), 0)
        < lax.broadcasted_iota(jnp.int32, (seq_count, seq_count), 1),
        1.0,
        0.0,
    )
    rank = jnp.dot(named, before, preferred_element_type=f32)
    mine = rank == slot
    return jnp.where(mine, named, 0.0), jnp.where(mine, weighted, 0.0)


def cell_kernel(
    slots, spans, paired,
    tokens_hbm, gain_hbm, next_gain_hbm, wq_hbm, wk_hbm, wv_hbm, wi_hbm, wf_hbm, bias_hbm, mem_hbm, norm_hbm,
    max_hbm, wo_hbm, ids_hbm, weights_hbm,
    partial_ref, keys_ref, values_ref, keep_ref, norm_out, max_out, placing_ref, mixing_ref, tokens_ref,
    next_gain_ref,
    gain_ref, wq_ref, wk_ref, wv_ref, wi_ref, wf_ref, bias_ref, mem_ref, norm_ref, max_ref, wo_ref, ids_ref,
    weights_ref, sems,
):
    pairs = (
        (tokens_hbm, tokens_ref), (gain_hbm, gain_ref), (ids_hbm, ids_ref), (weights_hbm, weights_ref),
        (wi_hbm, wi_ref), (wf_hbm, wf_ref), (bias_hbm, bias_ref), (max_hbm, max_ref), (norm_hbm, norm_ref),
        (wk_hbm, wk_ref), (wq_hbm, wq_ref), (mem_hbm, mem_ref), (wv_hbm, wv_ref), (wo_hbm, wo_ref),
        (next_gain_hbm, next_gain_ref),
    )
    copies = [pltpu.make_async_copy(a, b, sems.at[i]) for i, (a, b) in enumerate(pairs)]
    for copy in copies:
        copy.start()

    def arrive(first, last):
        for copy in copies[first:last]:
            copy.wait()

    head = lax.axis_index("tp")
    seq_count = tokens_ref.shape[0]
    head_dim = wq_ref.shape[1]
    arrive(0, 2)
    normed = scaled_tiles(tokens_ref[...].astype(f32), gain_ref)

    def project(ref):
        return jnp.dot(normed, ref[...], preferred_element_type=f32).astype(bf16).astype(f32)

    def gate(ref):
        return lax.dot_general(
            normed, ref[...], (((1,), (1,)), ((), ())), preferred_element_type=f32
        )

    arrive(2, 9)
    base = lax.axis_index("ep") if paired else 0
    shape = ids_ref[...], weights_ref[...], mixing_ref.shape[0], slots, spans, base
    placing, mixing = routing(*shape)
    if paired:
        placing, _ = routing(*shape, paired)
    placing_ref[...] = placing.astype(bf16)
    mixing_ref[...] = mixing
    inputs = gate(wi_ref)
    forgets = gate(wf_ref) + bias_ref[...]
    here = lax.broadcasted_iota(jnp.int32, inputs.shape, 1) == head
    input_gate = jnp.sum(jnp.where(here, inputs, 0.0), 1, keepdims=True)
    forget = jnp.sum(jnp.where(here, forgets, 0.0), 1, keepdims=True)
    forget_log = jnp.minimum(forget, 0.0) - jnp.log1p(jnp.exp(-jnp.abs(forget)))
    held = forget_log + to_column(max_ref[...])
    new_max = jnp.maximum(held, input_gate)
    keep = jnp.exp(held - new_max)
    fresh = jnp.exp(input_gate - new_max)
    max_out[...] = to_row(new_max)
    keep_ref[...] = jnp.broadcast_to(keep, keep_ref.shape)
    arrive(9, 10)
    key = project(wk_ref) * head_dim ** (-0.5)
    arrive(10, 11)
    query = project(wq_ref)
    query_t = query.T
    match = jnp.sum(query * key, 1, keepdims=True)
    new_norm = keep * norm_ref[...] + fresh * key
    norm_out[...] = new_norm
    keys_ref[...] = fresh * key
    denominator = jnp.sum(query * new_norm, 1, keepdims=True)
    scale = jnp.maximum(jnp.abs(denominator), jnp.exp(-new_max))
    arrive(11, 12)
    read = []
    for s in range(seq_count):
        read.append(jnp.sum(mem_ref[s] * query_t[:, s : s + 1], 0, keepdims=True))
    read = jnp.concatenate(read, 0)
    arrive(12, 13)
    value = project(wv_ref)
    values_ref[...] = value
    readout = (keep * read + (fresh * match) * value) / scale
    arrive(13, 14)
    partial_ref[...] = jnp.dot(
        readout.astype(bf16), wo_ref[...], preferred_element_type=f32
    ).astype(bf16)
    arrive(14, 15)


def pack_kernel(groups, tick_ref, tokens_ref, gain_ref, placing_ref, *refs):
    partials, outs, residual_ref = refs[: -groups - 1], refs[-groups - 1 : -1], refs[-1]
    total = partials[0][...].astype(f32)
    for ref in partials[1:]:
        total = total + ref[...].astype(f32)
    residual = (tokens_ref[...].astype(f32) + total).astype(bf16)
    residual_ref[...] = residual
    normed = scaled_tiles(residual.astype(f32), gain_ref)
    rows = jnp.dot(placing_ref[...], normed, preferred_element_type=f32).astype(bf16)
    if groups == 1:
        spread(rows, outs[0])
        return
    count, width = outs[0].shape[0], rows.shape[1]
    slots = outs[0].shape[1] // width
    for g, out_ref in enumerate(outs):
        for c in range(slots):
            start = (g * slots + c) * count
            out_ref[:, c * width : (c + 1) * width] = rows[start : start + count, :]


def spread(rows, out_ref):
    slots = out_ref.shape[1]
    for at in range(out_ref.shape[0]):
        out_ref[at] = rows[at * slots : (at + 1) * slots, :].astype(bf16)


def join_kernel(near_ref, far_ref, *outs):
    for at, out_ref in enumerate(outs):
        out_ref[0] = near_ref[at]
        out_ref[1] = far_ref[at]


def split_join_kernel(tick_ref, near_ref, far_ref, own_ref, first_ref, second_ref):
    near, far = near_ref[...].astype(f32), far_ref[...].astype(f32)

    def pair(at):
        return jnp.concatenate([near[at : at + 1, :], far[at : at + 1, :]], 0)

    odd = lax.axis_index("tp") & 1 == 1
    own_ref[...] = pair(0).astype(bf16)
    first_ref[...] = jnp.where(odd, pair(3), pair(1)).astype(bf16)
    second_ref[...] = pair(2).astype(bf16)


def fetch_kernel(tick_ref, source_ref, target_ref, sems):
    pieces = sems.shape[0]
    height = source_ref.shape[0] // pieces
    copies = []
    for at in range(pieces):
        rows = pl.ds(at * height, height)
        copies.append(
            pltpu.make_async_copy(source_ref.at[rows], target_ref.at[rows], sems.at[at])
        )
    for copy in copies:
        copy.start()
    for copy in copies:
        copy.wait()


def fetched(weight, after):
    return kernel_call(
        fetch_kernel,
        (pltpu.VMEM(weight.shape, weight.dtype),),
        (after, *in_hbm(weight)),
        in_specs=[ANY] * 2,
        out_specs=(ANY,),
        scratch=[pltpu.SemaphoreType.DMA((8,))],
        cost=20_000_000,
        limit=1 << 20,
    )[0]


def stacked(refs):
    return jnp.concatenate(
        [ref[at].astype(f32) for ref in refs for at in range(ref.shape[0])], 0
    )


def expert_kernel(*refs):
    *parts, gate_ref, up_ref, out_ref = refs
    deep = gate_ref.shape[0]
    if len(parts) == 1:
        rows = stacked(parts).astype(bf16)
    else:
        own, first, second, other_first = [ref[...].astype(f32) for ref in parts]
        odd = lax.axis_index("tp") & 1 == 1
        pieces = []
        for part in (
            own,
            jnp.where(odd, other_first, first),
            second,
            jnp.where(odd, first, other_first),
        ):
            pieces += [part[:, at : at + deep] for at in range(0, part.shape[1], deep)]
        rows = jnp.concatenate(pieces, 0).astype(bf16)
    width = out_ref.shape[1]
    step = min(width, 512)
    for at in range(0, width, step):
        gate_sum = jnp.dot(rows, gate_ref[:, at : at + step], preferred_element_type=f32)
        up_sum = jnp.dot(rows, up_ref[:, at : at + step], preferred_element_type=f32)
        out_ref[:, at : at + step] = (gate_sum * jax.nn.sigmoid(gate_sum) * up_sum).astype(bf16)


def down_term(hidden_ref, weight_ref, k):
    units = hidden_ref.shape[1]
    start = pl.multiple_of((lax.axis_index("tp") ^ k) * units, units)
    return jnp.dot(
        hidden_ref[...], weight_ref[pl.ds(start, units), :], preferred_element_type=f32
    )


def first_down_kernel(own_ref, weight_ref, total_ref):
    total_ref[...] = down_term(own_ref, weight_ref, 0)


def next_down_kernel(numbers, before_ref, *refs):
    *hiddens, weight_ref, total_ref = refs
    total = before_ref[...]
    for k, hidden_ref in zip(numbers, hiddens):
        total = total + down_term(hidden_ref, weight_ref, k)
    total_ref[...] = total


def down_kernel(total_ref, hidden_ref, weight_ref, *outs):
    total = total_ref[...] + down_term(hidden_ref, weight_ref, LATEST)
    if len(outs) == 1:
        spread(total, outs[0])
        return
    slots, count = outs[0].shape[1], len(outs)
    for g, out_ref in enumerate(outs):
        for at in range(out_ref.shape[0]):
            picked = [(at * slots + c) * count + g for c in range(slots)]
            out_ref[at] = jnp.concatenate([total[r : r + 1, :] for r in picked], 0).astype(bf16)


def state_kernel(tick_ref, mem_ref, keys_ref, values_ref, keep_ref, norm_ref, max_ref, out_ref, norm_out, max_out):
    norm_out[...] = norm_ref[...]
    max_out[...] = max_ref[...]
    keys_t = keys_ref[...].T
    value = values_ref[...]
    for s in range(mem_ref.shape[0]):
        out_ref[s] = (
            keep_ref[s : s + 1, :] * mem_ref[s] + keys_t[:, s : s + 1] * value[s : s + 1, :]
        )


def final_kernel(residual_ref, mixing_ref, *refs):
    *parts, out_ref = refs
    width = out_ref.shape[1]
    start = pl.multiple_of(lax.axis_index("tp") * width, width)
    weights = mixing_ref[...].T
    routed, at = None, 0
    for ref in parts:
        for place in range(ref.shape[0]):
            block = ref[place].astype(f32)
            for c in range(ref.shape[1]):
                term = weights[:, at : at + 1] * block[c : c + 1, :]
                routed = term if routed is None else routed + term
                at += 1
    out_ref[...] = (residual_ref[:, pl.ds(start, width)].astype(f32) + routed).astype(bf16)


def in_hbm(*values):
    return [pltpu.with_memory_space_constraint(value, pltpu.HBM) for value in values]


def swapped(value, axis, bits):
    count = lax.axis_size(axis)
    return lax.ppermute(value, axis, [(at, at ^ bits) for at in range(count)])


def sent(value, target):
    ep_count, tp_count = lax.axis_size("ep"), lax.axis_size("tp")
    pairs = []
    for e in range(ep_count):
        for t in range(tp_count):
            to_e, to_t = target(e, t)
            pairs.append((e * tp_count + t, to_e * tp_count + to_t))
    return lax.ppermute(value, ("ep", "tp"), pairs)


def from_partners(value, count):
    moved = [swapped(value, "tp", k) for k in reversed(range(1, count))]
    return [value, *reversed(moved)]


def gathered(near, far, w_up):
    came = swapped(far, "ep", 1)
    up_w = fetched(w_up, far)
    pair = (2, near.shape[1])
    own, first, second = kernel_call(
        split_join_kernel,
        tuple(pltpu.VMEM(pair, near.dtype) for _ in range(3)),
        (up_w, near, came),
        in_specs=[ANY, VMEM, VMEM],
        limit=4 << 20,
    )
    first = sent(first, lambda e, t: (e ^ 6, t) if t & 1 else (e ^ 2, t))
    second = sent(second, lambda e, t: (e ^ 4, t))
    return [own, first, second, swapped(first, "tp", 1)], up_w


def returned_blocks(near, far):
    came = swapped(far, "ep", 1)
    count, *block = near.shape
    joined = kernel_call(
        join_kernel,
        tuple(pltpu.VMEM((2, *block), near.dtype) for _ in range(count)),
        (near, came),
        limit=4 << 20,
    )
    moved = [swapped(joined[k], "ep", 2 * k) for k in reversed(range(1, count))]
    return [joined[0], *reversed(moved)], joined[1]


def shards(
    tokens, mix_gain, w_query, w_key, w_value, w_igate, w_fgate, forget_bias, w_out, mem_state, norm_state,
    max_state, ffn_gain, route_ids, route_weights, w_gate, w_up, w_down,
):
    seq_count, model_width = tokens.shape
    head_dim = norm_state.shape[1]
    tp_count = lax.axis_size("tp")
    ep_count = lax.axis_size("ep")
    own_width = model_width // tp_count
    top_count = route_ids.shape[1]
    spans = FF // w_down.shape[0]
    experts = ep_count // spans
    bound = max(2, 3 * seq_count * top_count // (2 * experts))
    slots = bound
    rows = ep_count * slots
    struct = jax.ShapeDtypeStruct
    direct = ep_count <= 8
    groups = 2 if direct else 1

    def block_outs(width):
        if direct:
            return tuple(pltpu.VMEM((ep_count // 2, slots, width), bf16) for _ in range(2))
        return (struct((ep_count, slots, width), bf16),)

    memory = mem_state.reshape(seq_count, head_dim, head_dim)
    gain_shape = (model_width // LANES, LANES)
    sources = (
        tokens, mix_gain.reshape(gain_shape), ffn_gain.reshape(gain_shape), w_query, w_key, w_value, w_igate.T,
        w_fgate.T, forget_bias.reshape(1, -1), memory, norm_state, max_state.T, w_out, route_ids.T,
        route_weights.T,
    )
    partial, keys, values, keep, new_norm, new_max, placing, mixing, rows_in, gain_b = kernel_call(
        functools.partial(cell_kernel, slots, spans, ep_count // 2 if direct else 0),
        (
            pltpu.VMEM((seq_count, model_width), bf16),
            pltpu.VMEM((seq_count, head_dim), f32),
            pltpu.VMEM((seq_count, head_dim), f32),
            pltpu.VMEM((seq_count, head_dim), f32),
            pltpu.VMEM((seq_count, head_dim), f32),
            pltpu.VMEM((1, seq_count), f32),
            pltpu.VMEM((rows, seq_count), bf16),
            pltpu.VMEM((rows, seq_count), f32),
            pltpu.VMEM((seq_count, model_width), bf16),
            pltpu.VMEM(gain_shape, bf16),
        ),
        in_hbm(*sources),
        in_specs=[ANY] * len(sources),
        scratch=[
            *(pltpu.VMEM(v.shape, v.dtype) for v in (sources[1], *sources[3:])),
            pltpu.SemaphoreType.DMA((len(sources),)),
        ],
        limit=16 << 20,
    )
    partials = from_partners(partial, tp_count)
    gate_w = fetched(w_gate, partial)
    if direct:
        packed_outs = [pltpu.VMEM((ep_count // 2, slots * model_width), bf16) for _ in range(2)]
    else:
        packed_outs = block_outs(model_width)
    *blocks, residual = kernel_call(
        functools.partial(pack_kernel, groups),
        (*packed_outs, pltpu.VMEM((seq_count, model_width), bf16)),
        (gate_w, rows_in, gain_b, placing, *partials),
        in_specs=[ANY] + [VMEM] * (3 + tp_count),
        limit=16 << 20,
    )
    if direct:
        arrived, up_w = gathered(*blocks, w_up)
    else:
        arrived = [lax.all_to_all(blocks[0], "ep", split_axis=0, concat_axis=0, tiled=True)]
        up_w = fetched(w_up, blocks[0])
    (hidden,) = kernel_call(
        expert_kernel,
        (pltpu.VMEM((rows, w_gate.shape[1]), bf16),),
        (*arrived, gate_w, up_w),
        limit=8 << 20,
    )
    hiddens = from_partners(hidden, tp_count)
    down_w = fetched(w_down, hidden)
    (total,) = kernel_call(
        first_down_kernel,
        (pltpu.VMEM((rows, own_width), f32),),
        (hidden, down_w),
        cost=2_000_000,
        limit=8 << 20,
    )
    middle = [k for k in reversed(range(1, tp_count)) if k != LATEST]
    (total,) = kernel_call(
        functools.partial(next_down_kernel, middle),
        (pltpu.VMEM((rows, own_width), f32),),
        (total, *(hiddens[k] for k in middle), down_w),
        cost=2_000_000,
        limit=8 << 20,
    )
    blocks = kernel_call(
        down_kernel,
        block_outs(own_width),
        (total, hiddens[LATEST], down_w),
        limit=8 << 20,
    )

    def state(tick):
        return kernel_call(
            state_kernel,
            (
                struct((seq_count, head_dim, head_dim), f32),
                struct((seq_count, head_dim), f32),
                struct((1, seq_count), f32),
            ),
            (tick, memory, keys, values, keep, new_norm, new_max),
            in_specs=[ANY] + [VMEM] * 6,
            cost=20_000_000,
            limit=8 << 20,
        )

    if direct:
        returned, tick = returned_blocks(*blocks)
    else:
        tick = blocks[0]
        returned = [lax.all_to_all(tick, "ep", split_axis=0, concat_axis=0, tiled=True)]
    new_memory, new_norm, new_max = state(tick)
    (out_tokens,) = kernel_call(
        final_kernel,
        (struct((seq_count, own_width), bf16),),
        (residual, mixing, *returned),
        limit=8 << 20,
    )
    return (
        out_tokens,
        new_memory.reshape(mem_state.shape),
        new_norm,
        new_max.T,
    )


def solution(mesh):
    placed = (
        P("ep", None),
        P(),
        P(None, "tp"),
        P(None, "tp"),
        P(None, "tp"),
        P(),
        P(),
        P(),
        P("tp", None),
        P("ep", "tp", None),
        P("ep", "tp"),
        P("ep", "tp"),
        P(),
        P("ep", None),
        P("ep", None),
        P(None, ("ep", "tp")),
        P(None, ("ep", "tp")),
        P("ep", "tp"),
    )

    return jax.shard_map(
        shards,
        mesh=mesh,
        in_specs=placed,
        out_specs=(P("ep", "tp"), P("ep", "tp", None), P("ep", "tp"), P("ep", "tp")),
        check_vma=False,
    )
```

```python
import functools
import jax
import jax.numpy as jnp
from jax import lax
from jax.experimental import pallas as pl
from jax.experimental.pallas import tpu as pltpu
from jax.sharding import PartitionSpec as P

FF = 4096
LATEST = 2
LANES = 128
epsilon = 1e-06
f32 = jnp.float32
bf16 = jnp.bfloat16


VMEM = pl.BlockSpec(memory_space=pltpu.VMEM)
ANY = pl.BlockSpec(memory_space=pl.ANY)


def kernel_call(body, outs, ins, in_specs=None, out_specs=None, scratch=(), cost=1000, limit=None):
    return pl.pallas_call(
        body,
        out_shape=outs,
        in_specs=in_specs or [VMEM] * len(ins),
        out_specs=out_specs or tuple([VMEM] * len(outs)),
        scratch_shapes=list(scratch),
        compiler_params=pltpu.CompilerParams(vmem_limit_bytes=limit),
        cost_estimate=pl.CostEstimate(flops=cost, bytes_accessed=0, transcendentals=0),
    )(*ins)


def scaled_tiles(wide, gain_ref):
    width = wide.shape[1]
    factor = lax.rsqrt(jnp.sum(wide * wide, 1, keepdims=True) / width + epsilon)
    gain = gain_ref[...].astype(f32)
    tiles = [
        wide[:, at * LANES : (at + 1) * LANES] * factor * gain[at : at + 1, :]
        for at in range(width // LANES)
    ]
    return jnp.concatenate(tiles, 1).astype(bf16)


def to_column(row):
    count = row.shape[1]
    eye = lax.broadcasted_iota(jnp.int32, (count, count), 0) == lax.broadcasted_iota(
        jnp.int32, (count, count), 1
    )
    return jnp.sum(jnp.where(eye, jnp.broadcast_to(row, (count, count)), 0.0), 1, keepdims=True)


def to_row(column):
    count = column.shape[0]
    eye = lax.broadcasted_iota(jnp.int32, (count, count), 0) == lax.broadcasted_iota(
        jnp.int32, (count, count), 1
    )
    return jnp.sum(jnp.where(eye, jnp.broadcast_to(column, (count, count)), 0.0), 0, keepdims=True)


def routing(ids, weights, rows, slots, spans, base, paired=0):
    top_count, seq_count = ids.shape
    at = lax.broadcasted_iota(jnp.int32, (rows, seq_count), 0)
    if paired:
        slot = (at // paired % slots).astype(f32)
        block = at % paired * 2 + at // (paired * slots)
    else:
        slot = (at % slots).astype(f32)
        block = at // slots
    expert = (block ^ base) // spans
    named = jnp.zeros((rows, seq_count), f32)
    weighted = jnp.zeros((rows, seq_count), f32)
    for k in range(top_count):
        hit = expert == ids[k : k + 1, :]
        named = named + jnp.where(hit, 1.0, 0.0)
        weighted = weighted + jnp.where(hit, weights[k : k + 1, :], 0.0)
    before = jnp.where(
        lax.broadcasted_iota(jnp.int32, (seq_count, seq_count), 0)
        < lax.broadcasted_iota(jnp.int32, (seq_count, seq_count), 1),
        1.0,
        0.0,
    )
    rank = jnp.dot(named, before, preferred_element_type=f32)
    mine = rank == slot
    return jnp.where(mine, named, 0.0), jnp.where(mine, weighted, 0.0)


def cell_kernel(
    slots, spans, paired,
    tokens_hbm, gain_hbm, next_gain_hbm, wq_hbm, wk_hbm, wv_hbm, wi_hbm, wf_hbm, bias_hbm, mem_hbm, norm_hbm,
    max_hbm, wo_hbm, ids_hbm, weights_hbm,
    partial_ref, keys_ref, values_ref, keep_ref, norm_out, max_out, placing_ref, mixing_ref, tokens_ref,
    next_gain_ref,
    gain_ref, wq_ref, wk_ref, wv_ref, wi_ref, wf_ref, bias_ref, mem_ref, norm_ref, max_ref, wo_ref, ids_ref,
    weights_ref, sems,
):
    pairs = (
        (tokens_hbm, tokens_ref), (gain_hbm, gain_ref), (ids_hbm, ids_ref), (weights_hbm, weights_ref),
        (wi_hbm, wi_ref), (wf_hbm, wf_ref), (bias_hbm, bias_ref), (max_hbm, max_ref), (norm_hbm, norm_ref),
        (wk_hbm, wk_ref), (wq_hbm, wq_ref), (wv_hbm, wv_ref), (mem_hbm, mem_ref), (wo_hbm, wo_ref),
        (next_gain_hbm, next_gain_ref),
    )
    copies = [pltpu.make_async_copy(a, b, sems.at[i]) for i, (a, b) in enumerate(pairs)]
    for copy in copies:
        copy.start()

    def arrive(first, last):
        for copy in copies[first:last]:
            copy.wait()

    head = lax.axis_index("tp")
    seq_count = tokens_ref.shape[0]
    head_dim = wq_ref.shape[1]
    arrive(0, 2)
    normed = scaled_tiles(tokens_ref[...].astype(f32), gain_ref)

    def project(ref):
        return jnp.dot(normed, ref[...], preferred_element_type=f32).astype(bf16).astype(f32)

    def gate(ref):
        return lax.dot_general(
            normed, ref[...], (((1,), (1,)), ((), ())), preferred_element_type=f32
        )

    arrive(2, 9)
    base = lax.axis_index("ep") if paired else 0
    shape = ids_ref[...], weights_ref[...], mixing_ref.shape[0], slots, spans, base
    placing, mixing = routing(*shape)
    if paired:
        placing, _ = routing(*shape, paired)
    placing_ref[...] = placing.astype(bf16)
    mixing_ref[...] = mixing
    inputs = gate(wi_ref)
    forgets = gate(wf_ref) + bias_ref[...]
    here = lax.broadcasted_iota(jnp.int32, inputs.shape, 1) == head
    input_gate = jnp.sum(jnp.where(here, inputs, 0.0), 1, keepdims=True)
    forget = jnp.sum(jnp.where(here, forgets, 0.0), 1, keepdims=True)
    forget_log = jnp.minimum(forget, 0.0) - jnp.log1p(jnp.exp(-jnp.abs(forget)))
    held = forget_log + to_column(max_ref[...])
    new_max = jnp.maximum(held, input_gate)
    keep = jnp.exp(held - new_max)
    fresh = jnp.exp(input_gate - new_max)
    max_out[...] = to_row(new_max)
    keep_ref[...] = jnp.broadcast_to(keep, keep_ref.shape)
    arrive(9, 10)
    key = project(wk_ref) * head_dim ** (-0.5)
    arrive(10, 11)
    query = project(wq_ref)
    query_t = query.T
    match = jnp.sum(query * key, 1, keepdims=True)
    new_norm = keep * norm_ref[...] + fresh * key
    norm_out[...] = new_norm
    keys_ref[...] = fresh * key
    denominator = jnp.sum(query * new_norm, 1, keepdims=True)
    scale = jnp.maximum(jnp.abs(denominator), jnp.exp(-new_max))
    arrive(11, 12)
    value = project(wv_ref)
    values_ref[...] = value
    arrive(12, 13)
    read = []
    for s in range(seq_count):
        read.append(jnp.sum(mem_ref[s] * query_t[:, s : s + 1], 0, keepdims=True))
    read = jnp.concatenate(read, 0)
    readout = (keep * read + (fresh * match) * value) / scale
    arrive(13, 14)
    partial_ref[...] = jnp.dot(
        readout.astype(bf16), wo_ref[...], preferred_element_type=f32
    ).astype(bf16)
    arrive(14, 15)


def pack_kernel(groups, tick_ref, tokens_ref, gain_ref, placing_ref, *refs):
    partials, outs, residual_ref = refs[: -groups - 1], refs[-groups - 1 : -1], refs[-1]
    total = partials[0][...].astype(f32)
    for ref in partials[1:]:
        total = total + ref[...].astype(f32)
    residual = (tokens_ref[...].astype(f32) + total).astype(bf16)
    residual_ref[...] = residual
    normed = scaled_tiles(residual.astype(f32), gain_ref)
    rows = jnp.dot(placing_ref[...], normed, preferred_element_type=f32).astype(bf16)
    if groups == 1:
        spread(rows, outs[0])
        return
    count, width = outs[0].shape[0], rows.shape[1]
    slots = outs[0].shape[1] // width
    for g, out_ref in enumerate(outs):
        for c in range(slots):
            start = (g * slots + c) * count
            out_ref[:, c * width : (c + 1) * width] = rows[start : start + count, :]


def spread(rows, out_ref):
    slots = out_ref.shape[1]
    for at in range(out_ref.shape[0]):
        out_ref[at] = rows[at * slots : (at + 1) * slots, :].astype(bf16)


def join_kernel(near_ref, far_ref, *outs):
    for at, out_ref in enumerate(outs):
        out_ref[0] = near_ref[at]
        out_ref[1] = far_ref[at]


def split_join_kernel(tick_ref, near_ref, far_ref, own_ref, first_ref, second_ref):
    near, far = near_ref[...].astype(f32), far_ref[...].astype(f32)

    def pair(at):
        return jnp.concatenate([near[at : at + 1, :], far[at : at + 1, :]], 0)

    odd = lax.axis_index("tp") & 1 == 1
    own_ref[...] = pair(0).astype(bf16)
    first_ref[...] = jnp.where(odd, pair(3), pair(1)).astype(bf16)
    second_ref[...] = pair(2).astype(bf16)


def fetch_kernel(tick_ref, source_ref, target_ref, sems):
    pieces = sems.shape[0]
    height = source_ref.shape[0] // pieces
    copies = []
    for at in range(pieces):
        rows = pl.ds(at * height, height)
        copies.append(
            pltpu.make_async_copy(source_ref.at[rows], target_ref.at[rows], sems.at[at])
        )
    for copy in copies:
        copy.start()
    for copy in copies:
        copy.wait()


def fetched(weight, after):
    return kernel_call(
        fetch_kernel,
        (pltpu.VMEM(weight.shape, weight.dtype),),
        (after, *in_hbm(weight)),
        in_specs=[ANY] * 2,
        out_specs=(ANY,),
        scratch=[pltpu.SemaphoreType.DMA((8,))],
        cost=20_000_000,
        limit=1 << 20,
    )[0]


def stacked(refs):
    return jnp.concatenate(
        [ref[at].astype(f32) for ref in refs for at in range(ref.shape[0])], 0
    )


def expert_kernel(*refs):
    *parts, gate_ref, up_ref, out_ref = refs
    deep = gate_ref.shape[0]
    if len(parts) == 1:
        rows = stacked(parts).astype(bf16)
    else:
        own, first, second, other_first = [ref[...].astype(f32) for ref in parts]
        odd = lax.axis_index("tp") & 1 == 1
        pieces = []
        for part in (
            own,
            jnp.where(odd, other_first, first),
            second,
            jnp.where(odd, first, other_first),
        ):
            pieces += [part[:, at : at + deep] for at in range(0, part.shape[1], deep)]
        rows = jnp.concatenate(pieces, 0).astype(bf16)
    width = out_ref.shape[1]
    step = min(width, 512)
    for at in range(0, width, step):
        gate_sum = jnp.dot(rows, gate_ref[:, at : at + step], preferred_element_type=f32)
        up_sum = jnp.dot(rows, up_ref[:, at : at + step], preferred_element_type=f32)
        out_ref[:, at : at + step] = (gate_sum * jax.nn.sigmoid(gate_sum) * up_sum).astype(bf16)


def down_term(hidden_ref, weight_ref, k):
    units = hidden_ref.shape[1]
    start = pl.multiple_of((lax.axis_index("tp") ^ k) * units, units)
    return jnp.dot(
        hidden_ref[...], weight_ref[pl.ds(start, units), :], preferred_element_type=f32
    )


def first_down_kernel(own_ref, weight_ref, total_ref):
    total_ref[...] = down_term(own_ref, weight_ref, 0)


def next_down_kernel(numbers, before_ref, *refs):
    *hiddens, weight_ref, total_ref = refs
    total = before_ref[...]
    for k, hidden_ref in zip(numbers, hiddens):
        total = total + down_term(hidden_ref, weight_ref, k)
    total_ref[...] = total


def down_kernel(total_ref, hidden_ref, weight_ref, *outs):
    total = total_ref[...] + down_term(hidden_ref, weight_ref, LATEST)
    if len(outs) == 1:
        spread(total, outs[0])
        return
    slots, count = outs[0].shape[1], len(outs)
    for g, out_ref in enumerate(outs):
        for at in range(out_ref.shape[0]):
            picked = [(at * slots + c) * count + g for c in range(slots)]
            out_ref[at] = jnp.concatenate([total[r : r + 1, :] for r in picked], 0).astype(bf16)


def state_kernel(tick_ref, mem_ref, keys_ref, values_ref, keep_ref, norm_ref, max_ref, out_ref, norm_out, max_out):
    norm_out[...] = norm_ref[...]
    max_out[...] = max_ref[...]
    keys_t = keys_ref[...].T
    value = values_ref[...]
    for s in range(mem_ref.shape[0]):
        out_ref[s] = (
            keep_ref[s : s + 1, :] * mem_ref[s] + keys_t[:, s : s + 1] * value[s : s + 1, :]
        )


def weighted(mixing_ref, parts):
    weights = mixing_ref[...].T
    total = None
    for number, ref in parts:
        count, slots, _ = ref.shape
        for place in range(count):
            block = ref[place].astype(f32)
            for c in range(slots):
                at = (number * count + place) * slots + c
                term = weights[:, at : at + 1] * block[c : c + 1, :]
                total = term if total is None else total + term
    return total


def early_kernel(numbers, residual_ref, mixing_ref, *refs):
    *parts, out_ref = refs
    width = out_ref.shape[1]
    start = pl.multiple_of(lax.axis_index("tp") * width, width)
    residual = residual_ref[:, pl.ds(start, width)].astype(f32)
    out_ref[...] = residual + weighted(mixing_ref, zip(numbers, parts))


def final_kernel(number, before_ref, mixing_ref, part_ref, out_ref):
    out_ref[...] = (before_ref[...] + weighted(mixing_ref, [(number, part_ref)])).astype(bf16)


def whole_kernel(residual_ref, mixing_ref, part_ref, out_ref):
    width = out_ref.shape[1]
    start = pl.multiple_of(lax.axis_index("tp") * width, width)
    residual = residual_ref[:, pl.ds(start, width)].astype(f32)
    out_ref[...] = (residual + weighted(mixing_ref, [(0, part_ref)])).astype(bf16)


def in_hbm(*values):
    return [pltpu.with_memory_space_constraint(value, pltpu.HBM) for value in values]


def swapped(value, axis, bits):
    count = lax.axis_size(axis)
    return lax.ppermute(value, axis, [(at, at ^ bits) for at in range(count)])


def sent(value, target):
    ep_count, tp_count = lax.axis_size("ep"), lax.axis_size("tp")
    pairs = []
    for e in range(ep_count):
        for t in range(tp_count):
            to_e, to_t = target(e, t)
            pairs.append((e * tp_count + t, to_e * tp_count + to_t))
    return lax.ppermute(value, ("ep", "tp"), pairs)


def from_partners(value, count):
    moved = [swapped(value, "tp", k) for k in reversed(range(1, count))]
    return [value, *reversed(moved)]


def gathered(near, far, w_up):
    came = swapped(far, "ep", 1)
    up_w = fetched(w_up, far)
    pair = (2, near.shape[1])
    own, first, second = kernel_call(
        split_join_kernel,
        tuple(pltpu.VMEM(pair, near.dtype) for _ in range(3)),
        (up_w, near, came),
        in_specs=[ANY, VMEM, VMEM],
        limit=4 << 20,
    )
    first = sent(first, lambda e, t: (e ^ 6, t) if t & 1 else (e ^ 2, t))
    second = sent(second, lambda e, t: (e ^ 4, t))
    return [own, first, second, swapped(first, "tp", 1)], up_w


def returned_blocks(near, far):
    came = swapped(far, "ep", 1)
    count, *block = near.shape
    joined = kernel_call(
        join_kernel,
        tuple(pltpu.VMEM((2, *block), near.dtype) for _ in range(count)),
        (near, came),
        limit=4 << 20,
    )
    moved = [swapped(joined[k], "ep", 2 * k) for k in reversed(range(1, count))]
    return [joined[0], *reversed(moved)], joined[1]


def shards(
    tokens, mix_gain, w_query, w_key, w_value, w_igate, w_fgate, forget_bias, w_out, mem_state, norm_state,
    max_state, ffn_gain, route_ids, route_weights, w_gate, w_up, w_down,
):
    seq_count, model_width = tokens.shape
    head_dim = norm_state.shape[1]
    tp_count = lax.axis_size("tp")
    ep_count = lax.axis_size("ep")
    own_width = model_width // tp_count
    top_count = route_ids.shape[1]
    spans = FF // w_down.shape[0]
    experts = ep_count // spans
    bound = max(2, 3 * seq_count * top_count // (2 * experts))
    slots = bound
    rows = ep_count * slots
    struct = jax.ShapeDtypeStruct
    direct = ep_count <= 8
    groups = 2 if direct else 1

    def block_outs(width):
        if direct:
            return tuple(pltpu.VMEM((ep_count // 2, slots, width), bf16) for _ in range(2))
        return (struct((ep_count, slots, width), bf16),)

    memory = mem_state.reshape(seq_count, head_dim, head_dim)
    gain_shape = (model_width // LANES, LANES)
    sources = (
        tokens, mix_gain.reshape(gain_shape), ffn_gain.reshape(gain_shape), w_query, w_key, w_value, w_igate.T,
        w_fgate.T, forget_bias.reshape(1, -1), memory, norm_state, max_state.T, w_out, route_ids.T,
        route_weights.T,
    )
    partial, keys, values, keep, new_norm, new_max, placing, mixing, rows_in, gain_b = kernel_call(
        functools.partial(cell_kernel, slots, spans, ep_count // 2 if direct else 0),
        (
            pltpu.VMEM((seq_count, model_width), bf16),
            pltpu.VMEM((seq_count, head_dim), f32),
            pltpu.VMEM((seq_count, head_dim), f32),
            pltpu.VMEM((seq_count, head_dim), f32),
            pltpu.VMEM((seq_count, head_dim), f32),
            pltpu.VMEM((1, seq_count), f32),
            pltpu.VMEM((rows, seq_count), bf16),
            pltpu.VMEM((rows, seq_count), f32),
            pltpu.VMEM((seq_count, model_width), bf16),
            pltpu.VMEM(gain_shape, bf16),
        ),
        in_hbm(*sources),
        in_specs=[ANY] * len(sources),
        scratch=[
            *(pltpu.VMEM(v.shape, v.dtype) for v in (sources[1], *sources[3:])),
            pltpu.SemaphoreType.DMA((len(sources),)),
        ],
        limit=16 << 20,
    )
    partials = from_partners(partial, tp_count)
    gate_w = fetched(w_gate, partial)
    if direct:
        packed_outs = [pltpu.VMEM((ep_count // 2, slots * model_width), bf16) for _ in range(2)]
    else:
        packed_outs = block_outs(model_width)
    *blocks, residual = kernel_call(
        functools.partial(pack_kernel, groups),
        (*packed_outs, pltpu.VMEM((seq_count, model_width), bf16)),
        (gate_w, rows_in, gain_b, placing, *partials),
        in_specs=[ANY] + [VMEM] * (3 + tp_count),
        limit=16 << 20,
    )
    if direct:
        arrived, up_w = gathered(*blocks, w_up)
    else:
        arrived = [lax.all_to_all(blocks[0], "ep", split_axis=0, concat_axis=0, tiled=True)]
        up_w = fetched(w_up, blocks[0])
    (hidden,) = kernel_call(
        expert_kernel,
        (pltpu.VMEM((rows, w_gate.shape[1]), bf16),),
        (*arrived, gate_w, up_w),
        limit=8 << 20,
    )
    hiddens = from_partners(hidden, tp_count)
    down_w = fetched(w_down, hidden)
    (total,) = kernel_call(
        first_down_kernel,
        (pltpu.VMEM((rows, own_width), f32),),
        (hidden, down_w),
        cost=2_000_000,
        limit=8 << 20,
    )
    middle = [k for k in reversed(range(1, tp_count)) if k != LATEST]
    (total,) = kernel_call(
        functools.partial(next_down_kernel, middle),
        (pltpu.VMEM((rows, own_width), f32),),
        (total, *(hiddens[k] for k in middle), down_w),
        cost=2_000_000,
        limit=8 << 20,
    )
    blocks = kernel_call(
        down_kernel,
        block_outs(own_width),
        (total, hiddens[LATEST], down_w),
        limit=8 << 20,
    )

    def state(tick):
        return kernel_call(
            state_kernel,
            (
                struct((seq_count, head_dim, head_dim), f32),
                struct((seq_count, head_dim), f32),
                struct((1, seq_count), f32),
            ),
            (tick, memory, keys, values, keep, new_norm, new_max),
            in_specs=[ANY] + [VMEM] * 6,
            cost=20_000_000,
            limit=8 << 20,
        )

    if direct:
        returned, tick = returned_blocks(*blocks)
    else:
        tick = blocks[0]
        returned = [lax.all_to_all(tick, "ep", split_axis=0, concat_axis=0, tiled=True)]
    new_memory, new_norm, new_max = state(tick)
    out_struct = struct((seq_count, own_width), bf16)
    if direct:
        last = 1
        numbers = [k for k in range(len(returned)) if k != last]
        (before,) = kernel_call(
            functools.partial(early_kernel, numbers),
            (pltpu.VMEM(out_struct.shape, f32),),
            (residual, mixing, *(returned[k] for k in numbers)),
            cost=2_000_000,
            limit=8 << 20,
        )
        (out_tokens,) = kernel_call(
            functools.partial(final_kernel, last),
            (out_struct,),
            (before, mixing, returned[last]),
            limit=8 << 20,
        )
    else:
        (out_tokens,) = kernel_call(
            whole_kernel, (out_struct,), (residual, mixing, *returned), limit=8 << 20
        )
    return (
        out_tokens,
        new_memory.reshape(mem_state.shape),
        new_norm,
        new_max.T,
    )


def solution(mesh):
    placed = (
        P("ep", None),
        P(),
        P(None, "tp"),
        P(None, "tp"),
        P(None, "tp"),
        P(),
        P(),
        P(),
        P("tp", None),
        P("ep", "tp", None),
        P("ep", "tp"),
        P("ep", "tp"),
        P(),
        P("ep", None),
        P("ep", None),
        P(None, ("ep", "tp")),
        P(None, ("ep", "tp")),
        P("ep", "tp"),
    )

    return jax.shard_map(
        shards,
        mesh=mesh,
        in_specs=placed,
        out_specs=(P("ep", "tp"), P("ep", "tp", None), P("ep", "tp"), P("ep", "tp")),
        check_vma=False,
    )
```
